256 devices in a mesh: sp: 64 (over z, y, core), tp: 4 (over x).
Axes of the slice: x: 4, y: 4, z: 8, core: 2. Of those that a mesh axis runs over, the one named last changes fastest.
Arguments:
- moe_input: bfloat16 [8192, 2048], P('sp', 'tp'), may hold values from -6 to 6
- cotangent: bfloat16 [8192, 2048], P('sp', 'tp'), may hold values from -16 to 16
- expert_ids: int32 [8192, 2], P('sp'), may hold values from 0 to 63, as said below
- routing_weights: float32 [8192, 2], P('sp'), may hold values from 0.1 to 0.6
- gate_weight: bfloat16 [64, 2048, 1024], P('sp', None, 'tp'), may hold values from -0.125 to 0.125
- up_weight: bfloat16 [64, 2048, 1024], P('sp', None, 'tp'), may hold values from -0.125 to 0.125
- down_weight: bfloat16 [64, 1024, 2048], P('sp', 'tp'), may hold values from -0.1875 to 0.1875
- inner_x: bfloat16 [8192, 4096], P('sp', 'tp'), may hold values from -6 to 6
- inner_b: bfloat16 [8192, 256], P('sp', 'tp'), may hold values from -6 to 6
- inner_c: bfloat16 [8192, 256], P('sp', 'tp'), may hold values from -6 to 6
- gate_z: bfloat16 [8192, 4096], P('sp', 'tp'), may hold values from -6 to 6
- step_raw: float32 [8192, 64], P('sp', 'tp'), may hold values from -30 to 2
- decay_rate: float32 [64], P('tp'), may hold values from 1 to 16
- skip_weight: float32 [64], P('tp'), may hold values from 0.1 to 1.9
- norm_gain: float32 [4096], P('tp'), may hold values from 0.1 to 1.9
- w_out: bfloat16 [2048, 4096], P(None, 'tp'), may hold values from -0.09375 to 0.09375
Outputs:
- gate_weight_gradient: bfloat16 [64, 2048, 1024], P('sp', None, 'tp')
- up_weight_gradient: bfloat16 [64, 2048, 1024], P('sp', None, 'tp')
- down_weight_gradient: bfloat16 [64, 1024, 2048], P('sp', 'tp')
- grad_out: float32 [2048, 4096], P('sp', 'tp')
- grad_inner_x: bfloat16 [8192, 4096], P('sp', 'tp')
- grad_inner_b: float32 [8192, 256], P('sp', 'tp')
- grad_inner_c: float32 [8192, 256], P('sp', 'tp')
- grad_gate_z: bfloat16 [8192, 4096], P('sp', 'tp')
- grad_step_raw: float32 [8192, 64], P('sp', 'tp')
The draws below stay inside these ranges and needn't reach their ends.
Inputs may be any that keep to these rules, and one draw needn't show every extreme that they name: `expert_ids`: the two entries of a row differ and lie in the same group of 16 consecutive experts. In each aligned block of 128 rows no expert is named more than 8 times; one group of experts, the same for all blocks, takes exactly half of every block's rows, and each of its experts is named exactly 8 times in every block.
All inputs are finite; a program needn't handle non-finite values.
Results may differ from the reference program's by a relative error of at most 0.015.
Values may be sent and summed in bfloat16 or wider, within the bound.
No kernel may reach another device: no remote copies, remote signals or barrier semaphores. Data moves between devices by JAX's collectives and lax.ppermute only.
A program may use at most 128 MiB of HBM per device.

```python
import math
from functools import partial
import jax
import jax.numpy as jnp
from jax import lax

D = 2048
HEADS = 64
HEAD_DIM = 64
GROUPS = 4
STATE = 64
SPAN = 128
FF = 1024
MOE_GROUPS = 4
TOP = 2
EXP_DEV = 1
TOKENS_PER_SHARD = 128
TOKENS = 8192
INNER = 4096
EXPERTS = 64
N_SP = 64
N_TP = 4


def head_laws(key):
    keys = jax.random.split(jax.random.fold_in(key, 101), 4)
    share = 0.5
    quick_head = jax.random.uniform(keys[0], (HEADS,), jnp.float32) < share
    decays = jnp.exp(jax.random.uniform(keys[1], (HEADS,), jnp.float32, 0.0, math.log(16.0)))
    quick = jnp.exp(jax.random.uniform(keys[2], (HEADS,), jnp.float32, math.log(1.0 / 120.0), math.log(1.0 / 40.0)))
    lasting = jnp.exp(jax.random.uniform(keys[3], (HEADS,), jnp.float32, math.log(0.1 / TOKENS), math.log(0.8 / TOKENS)))
    target = jnp.where(quick_head, quick, lasting)
    return (decays, target / decays)


def draw_decay_rate(key, part):
    return head_laws(key)[0]


def draw_step_raw(key, part):
    base_step = head_laws(key)[1]
    offsets = jnp.log(jnp.expm1(base_step))
    keys = jax.random.split(jax.random.fold_in(key, 202), 2)
    blocks = TOKENS // SPAN
    noise = jax.random.truncated_normal(keys[0], -2.5, 2.5, (TOKENS, HEADS), jnp.float32) * 0.7
    level = jax.random.uniform(keys[1], (blocks, 1, 1), jnp.float32, -0.7, 0.7)
    field = noise.reshape(blocks, SPAN, HEADS) + level
    return field.reshape(TOKENS, HEADS) + offsets[None, :]


def draw_expert_ids(key, part):
    expert_list = EXP_DEV * N_SP
    per_group = expert_list // MOE_GROUPS
    blocks = N_SP
    keys = jax.random.split(jax.random.fold_in(key, 303), 5)

    def shuffled(key_one):
        return jax.random.permutation(key_one, TOKENS_PER_SHARD)

    def mixed_table(key_one):
        return jax.random.permutation(key_one, per_group)
    full_group = jax.random.randint(keys[0], (), 0, MOE_GROUPS)
    order = jax.vmap(shuffled)(jax.random.split(keys[1], blocks))
    position = jnp.arange(TOKENS_PER_SHARD, dtype=jnp.int32)
    others = (full_group + 1 + jax.random.randint(keys[2], (blocks, TOKENS_PER_SHARD), 0, MOE_GROUPS - 1)) % MOE_GROUPS
    group_at = jnp.where(position[None, :] < TOKENS_PER_SHARD // 2, full_group, others).astype(jnp.int32)
    onehot = (group_at[:, :, None] == jnp.arange(MOE_GROUPS, dtype=jnp.int32)[None, None, :]).astype(jnp.int32)
    ranks = jnp.sum((jnp.cumsum(onehot, axis=1) - onehot) * onehot, axis=2)
    routing_tables = jax.vmap(mixed_table)(jax.random.split(keys[3], blocks * MOE_GROUPS)).reshape(blocks, MOE_GROUPS, per_group)
    offsets = jax.random.randint(keys[4], (blocks, MOE_GROUPS), 1, per_group)
    table_at = jnp.take_along_axis(routing_tables, jnp.broadcast_to(group_at[:, :, None], (blocks, TOKENS_PER_SHARD, per_group)), axis=1)
    shift_at = jnp.take_along_axis(offsets, group_at, axis=1)
    first = jnp.take_along_axis(table_at, (ranks % per_group)[:, :, None], axis=2)[:, :, 0]
    second = jnp.take_along_axis(table_at, ((ranks + shift_at) % per_group)[:, :, None], axis=2)[:, :, 0]
    chosen = jnp.stack([first, second], axis=2) + group_at[:, :, None] * per_group
    row_index = jnp.arange(blocks, dtype=jnp.int32)[:, None]
    placed = jnp.zeros((blocks, TOKENS_PER_SHARD, TOP), jnp.int32).at[row_index, order].set(chosen)
    return placed.reshape(blocks * TOKENS_PER_SHARD, TOP)


def strengthened(values, key, source, target, shards_of, factor):
    def block_of(dim):
        return (jnp.arange(values.shape[dim]) // (values.shape[dim] // shards_of)).reshape((-1,) + (1,) * (values.ndim - 1 - dim))

    near = jax.random.permutation(key, shards_of)[block_of(target)]
    second = (block_of(target) + shards_of // 2) % shards_of
    return jnp.where((block_of(source) == near) | (block_of(source) == second), factor * values, values)


def steps_of(stream_key, shape, pieces, smallest, top_value):
    gain, own = 1.0, jax.random.fold_in(stream_key, 6)
    for dim, blocks in pieces:
        draws = jnp.exp(jax.random.uniform(jax.random.fold_in(own, dim), (blocks,), jnp.float32, smallest / len(pieces), top_value / len(pieces)))
        gain = gain * jnp.repeat(draws, shape[dim] // blocks).reshape([-1 if axis == dim else 1 for axis in range(len(shape))])
    return gain


def gaussian(stream_key, dims, deviation, reach, cuts=(), held_as=jnp.bfloat16):
    array = deviation * jax.random.normal(stream_key, dims, jnp.float32)
    if cuts:
        array = array * steps_of(stream_key, dims, cuts, -0.22, 0.18)
    return jnp.clip(array, -reach, reach).astype(held_as)


def noise_with(key, dims, spread, reach, cuts, heavy, kind=jnp.bfloat16):
    array = spread * jax.random.normal(key, dims, jnp.float32)
    if cuts:
        array = array * steps_of(key, dims, cuts, -0.22, 0.18)
    return jnp.clip(strengthened(array, jax.random.fold_in(key, 3), *heavy), -reach, reach).astype(kind)


def setup_inputs(seed: int = 0) -> dict:
    streams_of = jax.random.split(jax.random.key(seed), 17)
    moe_input = gaussian(streams_of[0], (TOKENS, D), 1.0, 6.0, ((0, 64), (1, 4)))
    cotangent = noise_with(streams_of[1], (TOKENS, D), 1.0, 16.0, ((0, 64), (1, 4)), (0, 1, 64, 4.0))
    expert_ids = draw_expert_ids(jax.random.fold_in(streams_of[16], 71), 0)
    routing_weights = jnp.clip(0.1 + 0.5 * jax.random.uniform(streams_of[3], (TOKENS, TOP), jnp.float32) ** steps_of(streams_of[3], (TOKENS, TOP), ((0, 64),), -0.2, 0.2), 0.1, 0.6)
    gate_weight = gaussian(streams_of[4], (EXPERTS, D, FF), D ** -0.5, 0.125, ((0, 64), (2, 4)))
    up_weight = gaussian(streams_of[5], (EXPERTS, D, FF), D ** -0.5, 0.125, ((0, 64), (2, 4)))
    down_weight = gaussian(streams_of[6], (EXPERTS, FF, D), FF ** -0.5, 0.1875, ((0, 64), (1, 4)))
    inner_x = gaussian(streams_of[7], (TOKENS, INNER), 1.0, 6.0, ((0, 64), (1, 4)))
    inner_b = gaussian(streams_of[8], (TOKENS, GROUPS * STATE), 1.0, 6.0, ((0, 64), (1, 4)))
    inner_c = gaussian(streams_of[9], (TOKENS, GROUPS * STATE), 1.0, 6.0, ((0, 64), (1, 4)))
    gate_z = gaussian(streams_of[10], (TOKENS, INNER), 1.0, 6.0, ((0, 64), (1, 4)))
    step_raw = draw_step_raw(jax.random.fold_in(streams_of[16], 71), 0)
    decay_rate = draw_decay_rate(jax.random.fold_in(streams_of[16], 71), 0)
    skip_weight = jnp.clip(1.0 + 0.18 * jax.random.normal(streams_of[13], (HEADS,), jnp.float32), 0.1, 1.9)
    norm_gain = jnp.clip(1.0 + 0.18 * jax.random.normal(streams_of[14], (INNER,), jnp.float32), 0.1, 1.9)
    w_out = gaussian(streams_of[15], (D, INNER), INNER ** -0.5, 0.09375, ((1, 4),))
    return dict(moe_input=moe_input, cotangent=cotangent, expert_ids=expert_ids, routing_weights=routing_weights, gate_weight=gate_weight, up_weight=up_weight, down_weight=down_weight, inner_x=inner_x, inner_b=inner_b, inner_c=inner_c, gate_z=gate_z, step_raw=step_raw, decay_rate=decay_rate, skip_weight=skip_weight, norm_gain=norm_gain, w_out=w_out)


EPS = 0.01
HIGH = lax.Precision.HIGHEST

def slot_positions(chosen, expert_list, expert_capacity):
    listed = chosen.reshape(-1)
    onehot = (listed[:, None] == jnp.arange(expert_list, dtype=jnp.int32)[None, :]).astype(jnp.int32)
    before = jnp.cumsum(onehot, axis=0) - onehot
    return listed * expert_capacity + lax.optimization_barrier(jnp.sum(before * onehot, axis=1))

def prepare(inner_x32, inner_b32, step_raw, decays):
    tok_rows = inner_x32.shape[0]
    heads = decays.shape[0]
    groups = inner_b32.shape[1] // STATE
    per_group = heads // groups
    blocks = tok_rows // SPAN
    x_act = jax.nn.silu(inner_x32).reshape(tok_rows, heads, HEAD_DIM)
    b_blocks = jax.nn.silu(inner_b32).reshape(blocks, SPAN, groups, STATE)
    step_size = jax.nn.softplus(step_raw)
    decay_log = (-step_size * decays[None, :]).reshape(blocks, SPAN, groups, per_group)
    scaled = (x_act * step_size[:, :, None]).reshape(blocks, SPAN, groups, per_group, HEAD_DIM)
    return (x_act, b_blocks, decay_log, scaled)

def block_outputs(carry_state, block_in):
    x_block, log_block, b_block, c_block = block_in
    span_len = x_block.shape[0]
    running = jnp.cumsum(log_block, axis=0)
    places = jnp.arange(span_len)
    causal = (places[:, None] >= places[None, :])[:, :, None, None]
    between = running[:, None] - running[None, :]
    weights = jnp.where(causal, jnp.exp(jnp.where(causal, between, 0.0)), 0.0)
    scores = jnp.einsum('lgn,sgn->lsg', c_block, b_block, precision=HIGH)
    inside = jnp.einsum('lsg,lsge,sgep->lgep', scores, weights, x_block, precision=HIGH)
    carried = jnp.einsum('lgn,gepn,lge->lgep', c_block, carry_state, jnp.exp(running), precision=HIGH)
    to_end = jnp.exp(running[-1] - running)
    fresh_state = jnp.einsum('lgn,lge,lgep->gepn', b_block, to_end, x_block, precision=HIGH)
    return (carry_state * jnp.exp(running[-1])[:, :, None, None] + fresh_state, inside + carried)

def mixer_output(inner_x32, inner_b32, inner_c32, gate_z32, step_raw, carry_in, decays, skip_weight, norm_gain):
    tok_rows = inner_x32.shape[0]
    heads = decays.shape[0]
    groups = inner_b32.shape[1] // STATE
    x_act, b_blocks, decay_log, scaled = prepare(inner_x32, inner_b32, step_raw, decays)
    c_blocks = jax.nn.silu(inner_c32).reshape(tok_rows // SPAN, SPAN, groups, STATE)
    outputs = lax.scan(block_outputs, carry_in, (scaled, decay_log, b_blocks, c_blocks))[1]
    mixed_out = outputs.reshape(tok_rows, heads, HEAD_DIM) + x_act * skip_weight[None, :, None]
    gated_out = mixed_out.reshape(tok_rows, heads * HEAD_DIM) * jax.nn.silu(gate_z32)
    grouped = gated_out.reshape(tok_rows, groups, -1)
    normed = grouped * lax.rsqrt(lax.optimization_barrier(jnp.mean(grouped * grouped, axis=2, keepdims=True)) + EPS)
    return normed.reshape(tok_rows, -1) * norm_gain[None, :]

def expert_backward(padded_input, padded_gradient, item):
    owner, scaling, gate_w, up_w, down_w = item
    rows_in = padded_input[owner]
    rows_grad = (padded_gradient[owner].astype(jnp.float32) * scaling[:, None]).astype(jnp.bfloat16)
    gate_pre = jnp.dot(rows_in, gate_w, preferred_element_type=jnp.float32)
    up_pre = jnp.dot(rows_in, up_w, preferred_element_type=jnp.float32)
    sigmoid_gate = jax.nn.sigmoid(gate_pre)
    active = gate_pre * sigmoid_gate
    hidden = (active * up_pre).astype(jnp.bfloat16)
    hidden_grad = jnp.dot(rows_grad, down_w.T, preferred_element_type=jnp.float32)
    gate_grad = (hidden_grad * up_pre * sigmoid_gate * (1.0 + gate_pre * (1.0 - sigmoid_gate))).astype(jnp.bfloat16)
    up_grad = (hidden_grad * active).astype(jnp.bfloat16)
    down_part = jnp.dot(hidden.T, rows_grad, preferred_element_type=jnp.float32).astype(jnp.bfloat16)
    gate_part = jnp.dot(rows_in.T, gate_grad, preferred_element_type=jnp.float32).astype(jnp.bfloat16)
    up_part = jnp.dot(rows_in.T, up_grad, preferred_element_type=jnp.float32).astype(jnp.bfloat16)
    width = gate_w.shape[1] // N_TP
    summed = jnp.zeros(rows_in.shape, jnp.float32)
    for quarter in range(N_TP):
        low_col = quarter * width
        term = jnp.dot(gate_grad[:, low_col:low_col + width], gate_w[:, low_col:low_col + width].T, preferred_element_type=jnp.float32)
        term = term + jnp.dot(up_grad[:, low_col:low_col + width], up_w[:, low_col:low_col + width].T, preferred_element_type=jnp.float32)
        summed = summed + lax.optimization_barrier(term.astype(jnp.bfloat16)).astype(jnp.float32)
    return (gate_part, up_part, down_part, summed.astype(jnp.bfloat16))

def reference(moe_input, cotangent, expert_ids, routing_weights, gate_weight, up_weight, down_weight, inner_x, inner_b, inner_c, gate_z, step_raw, decay_rate, skip_weight, norm_gain, w_out):
    expert_list = gate_weight.shape[0]
    chosen_count = expert_ids.shape[1]
    expert_capacity = 4 * TOKENS_PER_SHARD // expert_list
    width = moe_input.shape[1]
    place_into_slots = jax.vmap(partial(slot_positions, expert_list=expert_list, expert_capacity=expert_capacity))(expert_ids.reshape(N_SP, TOKENS_PER_SHARD, chosen_count))
    local_owner = jnp.arange(TOKENS_PER_SHARD * chosen_count, dtype=jnp.int32) // chosen_count

    def routing_tables(spots, weights_block, block_index):
        owner = jnp.full((expert_list * expert_capacity,), TOKENS, jnp.int32).at[spots].set(local_owner + block_index * TOKENS_PER_SHARD)
        scaling = jnp.zeros((expert_list * expert_capacity,), jnp.float32).at[spots].set(weights_block)
        return (owner, scaling)
    owning_experts, scale_factors = jax.vmap(routing_tables)(place_into_slots, routing_weights.reshape(N_SP, TOKENS_PER_SHARD * chosen_count), jnp.arange(N_SP, dtype=jnp.int32))
    owning_experts = owning_experts.reshape(N_SP, expert_list, expert_capacity).transpose(1, 0, 2).reshape(expert_list, N_SP * expert_capacity)
    scale_factors = scale_factors.reshape(N_SP, expert_list, expert_capacity).transpose(1, 0, 2).reshape(expert_list, N_SP * expert_capacity)
    padded_input = jnp.concatenate([moe_input, jnp.zeros((1, width), jnp.bfloat16)], axis=0)
    padded_gradient = jnp.concatenate([cotangent, jnp.zeros((1, width), jnp.bfloat16)], axis=0)
    gate_weight_gradient, up_weight_gradient, down_weight_gradient, slot_gradient = lax.map(partial(expert_backward, padded_input, padded_gradient), (owning_experts, scale_factors, gate_weight, up_weight, down_weight))
    by_block = slot_gradient.reshape(expert_list, N_SP, expert_capacity, width).transpose(1, 0, 2, 3).reshape(N_SP, expert_list * expert_capacity, width)

    def collect(rows_block, spots):
        return rows_block[spots].astype(jnp.float32)
    moe_grad = lax.optimization_barrier(jnp.sum(jax.vmap(collect)(by_block, place_into_slots).reshape(TOKENS, chosen_count, width), axis=1))
    mixer_grad = (cotangent.astype(jnp.float32) + moe_grad).astype(jnp.bfloat16)
    groups = inner_b.shape[1] // STATE
    per_group = decay_rate.shape[0] // groups
    zero_state = jnp.zeros((groups, per_group, HEAD_DIM, STATE), jnp.float32)

    def forward(x_in, b_in, c_in, z_in, raw_in):
        return mixer_output(x_in, b_in, c_in, z_in, raw_in, zero_state, decay_rate, skip_weight, norm_gain)
    normed, pullback = jax.vjp(forward, inner_x.astype(jnp.float32), inner_b.astype(jnp.float32), inner_c.astype(jnp.float32), gate_z.astype(jnp.float32), step_raw)
    norm_out = normed.astype(jnp.bfloat16)
    grad_out = jnp.dot(mixer_grad.T, norm_out, preferred_element_type=jnp.float32)
    norm_grad = jnp.dot(mixer_grad, w_out, preferred_element_type=jnp.float32)
    x_grad, b_grad, c_grad, z_grad, raw_grad = pullback(norm_grad)
    return (gate_weight_gradient, up_weight_gradient, down_weight_gradient, grad_out, x_grad.astype(jnp.bfloat16), b_grad, c_grad, z_grad.astype(jnp.bfloat16), raw_grad)
```

```python
import jax
import jax.numpy as jnp
from jax import lax
from jax.sharding import Mesh
from jax.experimental import pallas as pl
from jax.experimental.pallas import tpu as pltpu
from jax.sharding import PartitionSpec as P

HEAD_DIM = 64
STATE = 64
LANES = 128
SLOTS = 8
EPS = 0.01
SP = ("z", "y", "c")
F32 = jnp.float32
BF16 = jnp.bfloat16
HIGH = lax.Precision.HIGHEST


def shifted(value, step):
    count = lax.axis_size("x")
    return lax.ppermute(value, "x", [(i, (i + step) % count) for i in range(count)])


def to_all(value, axes):
    return lax.all_to_all(value, axes, split_axis=0, concat_axis=0, tiled=True)


def placed(pieces, where):
    out = jnp.zeros((4, *pieces[0].shape), pieces[0].dtype)
    for piece, index in zip(pieces, where):
        out = lax.dynamic_update_index_in_dim(out, piece, index, 0)
    return out


def gathered_x(value):
    mine = lax.axis_index("x")
    half = value.shape[0] // 2
    left, right = shifted(value, 1), shifted(value, -1)
    far = jnp.concatenate([shifted(left[:half], 1), shifted(right[half:], -1)], axis=0)
    return placed(
        (value, left, right, far),
        (mine, (mine + 3) % 4, (mine + 1) % 4, (mine + 2) % 4),
    )


def summed_x(terms):
    mine = lax.axis_index("x")
    half = terms.shape[1] // 2

    def term(offset):
        return lax.dynamic_index_in_dim(terms, (mine + offset) % 4, 0, keepdims=False)

    far = term(2)
    from_left = shifted(far[:half], 1)
    from_right = shifted(far[half:], -1)
    up, down = term(1), term(3)
    up = jnp.concatenate(
        [(up[:half].astype(F32) + from_left.astype(F32)).astype(BF16), up[half:]], axis=0
    )
    down = jnp.concatenate(
        [down[:half], (down[half:].astype(F32) + from_right.astype(F32)).astype(BF16)], axis=0
    )
    low, high = shifted(up, 1), shifted(down, -1)
    return (term(0).astype(F32) + low.astype(F32) + high.astype(F32)).astype(BF16)


def rows_of(tiled):
    cols = tiled.shape[1] // SLOTS
    rows = tiled.reshape(-1, cols, SLOTS, LANES).transpose(0, 2, 1, 3)
    return rows.reshape(-1, cols * LANES)


SMALL, LARGE = 1 << 30, 1 << 32


def softplus(value):
    small = jnp.exp(-jnp.abs(value))
    grown = 1.0 + small
    log_part = jnp.where(
        grown == 1.0, small, jnp.log(grown) * (small / jnp.where(grown == 1.0, 1.0, grown - 1.0))
    )
    return jnp.maximum(value, 0.0) + log_part


def sigmoid(value):
    return 1.0 / (1.0 + jnp.exp(-value))


def mm(left, right):
    return jnp.dot(left.astype(BF16), right.astype(BF16), preferred_element_type=F32)


def mm_nt(left, right):
    return lax.dot_general(
        left.astype(BF16),
        right.astype(BF16),
        (((1,), (1,)), ((), ())),
        preferred_element_type=F32,
    )


def exact(left, right):
    return jnp.dot(left, right, preferred_element_type=F32, precision=HIGH)


def iota(shape, dim):
    return lax.broadcasted_iota(jnp.int32, shape, dim)


def head_lanes(heads, wide):
    return ((iota((heads, wide), 1) >> 6) == iota((heads, wide), 0)).astype(F32)


def head_rows(heads, wide):
    return ((iota((wide, heads), 0) >> 6) == iota((wide, heads), 1)).astype(F32)


def clocks(raw_t, rate):
    step = softplus(raw_t).T
    logs = -step * rate
    tok = logs.shape[0]
    upto = (iota((tok, tok), 0) >= iota((tok, tok), 1)).astype(F32)
    return step, exact(upto, logs)


def routing(ids_t, experts):
    numbers = iota((experts, ids_t.shape[1]), 0)
    first, second = ids_t[0:1, :] == numbers, ids_t[1:2, :] == numbers
    named = jnp.where(first, 1.0, jnp.where(second, 1.0, 0.0))
    tok = ids_t.shape[1]
    earlier = (iota((tok, tok), 0) < iota((tok, tok), 1)).astype(F32)
    before = mm(named, earlier)
    key = jnp.where(named > 0.0, before, -1.0)
    shape = (experts, SLOTS, tok)
    pick = jnp.broadcast_to(key[:, None, :], shape) == iota(shape, 1).astype(F32)
    return first, second, jnp.where(pick, 1.0, 0.0)


def put_tiles(out_ref, rows, experts):
    cols = rows.shape[1] // LANES
    tiled = rows.reshape(experts, SLOTS, rows.shape[1])
    for col in range(cols):
        out_ref[:, col * SLOTS : (col + 1) * SLOTS, :] = tiled[
            :, :, col * LANES : (col + 1) * LANES
        ].astype(BF16)


def put_pieces(out_ref, at, state):
    rows = state.shape[0] // 8
    for col in range(state.shape[1] // LANES):
        piece = state[:, col * LANES : (col + 1) * LANES].reshape(rows, 8, LANES)
        out_ref[col * rows : (col + 1) * rows, at : at + 8, :] = piece.astype(BF16)


def get_pieces(pieces):
    rows = STATE // 8
    cols = pieces.shape[0] // rows
    return jnp.concatenate(
        [pieces[col * rows : (col + 1) * rows].reshape(STATE, LANES) for col in range(cols)],
        axis=1,
    )


def enter_kernel(ids_ref, moe_ref, x_ref, b_ref, raw_ref, rate_ref, out_ref):
    experts = out_ref.shape[0]
    pick = routing(ids_ref[...], experts)[2]
    rows = mm(pick.reshape(experts * SLOTS, -1), moe_ref[...])
    put_tiles(out_ref, rows, experts)
    step, running = clocks(raw_ref[...], rate_ref[...])
    heads, wide = step.shape[1], x_ref.shape[1]
    last = running[-1:, :]
    spread = exact(
        jnp.concatenate(
            [step * jnp.exp(last - running), jnp.broadcast_to(jnp.exp(last), (8, heads))], axis=0
        ),
        head_lanes(heads, wide),
    )
    x = x_ref[...].astype(F32)
    at_end = x * sigmoid(x) * spread[:-8]
    b = b_ref[...].astype(F32)
    put_pieces(out_ref, 32, mm(b * sigmoid(b), at_end))
    total = spread[-8:]
    high = total.astype(BF16).astype(F32)
    mid = (total - high).astype(BF16).astype(F32)
    low = total - high - mid
    row = iota(total.shape, 0)
    tile = jnp.where(row == 0, high, jnp.where(row == 1, mid, jnp.where(row == 2, low, 0.0)))
    rows_at = STATE // 8
    for col in range(wide // LANES):
        part = tile[:, col * LANES : (col + 1) * LANES].astype(BF16)
        out_ref[col * rows_at : (col + 1) * rows_at, 40:48, :] = jnp.broadcast_to(
            part[None], (rows_at, 8, LANES)
        )


def weigh_kernel(ids_ref, weights_ref, cot_ref, out_ref):
    experts = out_ref.shape[0]
    first, second, pick = routing(ids_ref[...], experts)
    weights = weights_ref[...]
    weight_at = jnp.where(first, weights[0:1, :], 0.0) + jnp.where(second, weights[1:2, :], 0.0)
    scaling = jnp.sum(
        pick * jnp.broadcast_to(weight_at[:, None, :], pick.shape), axis=2, keepdims=True
    )
    rows = mm(pick.reshape(experts * SLOTS, -1), cot_ref[...])
    put_tiles(
        out_ref,
        (rows.reshape(experts, SLOTS, -1) * scaling).reshape(experts * SLOTS, -1),
        experts,
    )


def block_decays(got_ref):
    tile = got_ref[:, 40:48, :].astype(F32)
    total = tile[:, 0:1, :] + tile[:, 1:2, :] + tile[:, 2:3, :]
    return jnp.broadcast_to(total, tile.shape)


def ahead_kernel(got_ref, rows_ref, out_ref):
    out_ref[:, :32, :] = rows_ref[...]
    decays = block_decays(got_ref)
    pieces = got_ref[:, 32:40, :].astype(F32)
    total = jnp.zeros(pieces.shape[1:], F32)
    found = []
    for k in range(pieces.shape[0]):
        found.append(total)
        total = total * decays[k] + pieces[k]
    out_ref[:, 32:40, :] = jnp.stack(found, axis=0).astype(BF16)


def behind_kernel(got_ref, pieces_ref, out_ref):
    decays = block_decays(got_ref)
    pieces = pieces_ref[...].astype(F32)
    total = jnp.zeros(pieces.shape[1:], F32)
    found = []
    for k in reversed(range(pieces.shape[0])):
        found.append(total)
        total = total * decays[k] + pieces[k]
    out_ref[...] = jnp.stack(found[::-1], axis=0).astype(BF16)


def combine_kernel(ids_ref, cot_ref, back_ref, out_ref):
    experts = back_ref.shape[0] // SLOTS
    pick = routing(ids_ref[...], experts)[2].reshape(experts * SLOTS, -1)
    moe_grad = mm(pick.T, back_ref[...])
    rows = (cot_ref[...].astype(F32) + moe_grad).astype(BF16)
    for k in range(out_ref.shape[0]):
        out_ref[k] = rows


def halves(value):
    low = iota(value.shape, 1) < HEAD_DIM
    return jnp.where(low, value, 0.0), jnp.where(low, 0.0, value)


def fade_of(column, row, keep):
    return jnp.exp(jnp.where(keep, column - row, -1e30))


def forward_kernel(
    x_ref, z_ref, b_ref, c_ref, raw_ref, rate_ref, skip_ref, gain_ref, got_ref,
    norm_ref, mixed_ref, start_ref, wide_ref,
):
    start = get_pieces(got_ref[:, 32:40, :].astype(F32))
    start_ref[...] = start.astype(BF16)
    step, running = clocks(raw_ref[...], rate_ref[...])
    tok, heads = step.shape
    wide = x_ref.shape[1]
    spread = exact(
        jnp.concatenate(
            [step, jnp.exp(running), jnp.broadcast_to(skip_ref[...], (8, heads))], axis=0
        ),
        head_lanes(heads, wide),
    )
    x = x_ref[...].astype(F32)
    x_act = x * sigmoid(x)
    scaled = x_act * spread[:tok]
    wide_ref[...] = spread[tok : 2 * tok]
    b, c = b_ref[...].astype(F32), c_ref[...].astype(F32)
    b_t, c_t = b * sigmoid(b), c * sigmoid(c)
    c_act = c_t.T
    scores = mm(c_act, b_t)
    mixed = spread[tok : 2 * tok] * mm(c_act, start) + x_act * spread[2 * tok : 2 * tok + 1]
    running_t = running.T
    keep = iota((tok, tok), 0) >= iota((tok, tok), 1)
    for pair in range(heads // 2):
        lanes = slice(pair * LANES, (pair + 1) * LANES)
        mixes = [
            scores * fade_of(running[:, h : h + 1], running_t[h : h + 1, :], keep)
            for h in (2 * pair, 2 * pair + 1)
        ]
        inside = mm(
            jnp.concatenate(mixes, axis=1), jnp.concatenate(halves(scaled[:, lanes]), axis=0)
        )
        mixed_ref[:, lanes] = mixed[:, lanes] + inside
    z = z_ref[...].astype(F32)
    gated = mixed_ref[...] * (z * sigmoid(z))
    scale = lax.rsqrt(jnp.mean(gated * gated, axis=1, keepdims=True) + EPS)
    norm_ref[...] = (gated * scale * gain_ref[...]).astype(BF16)


def gate_back_kernel(
    grad_ref, mixed_ref, z_ref, gain_ref, wide_ref, c_ref, pieces_ref, grad_z_ref, d_mixed_ref
):
    z = z_ref[...].astype(F32)
    sig = sigmoid(z)
    z_act = z * sig
    mixed = mixed_ref[...]
    gated = mixed * z_act
    scale = lax.rsqrt(jnp.mean(gated * gated, axis=1, keepdims=True) + EPS)
    d_norm = grad_ref[...] * gain_ref[...]
    along = jnp.mean(d_norm * gated, axis=1, keepdims=True)
    d_gated = scale * d_norm - gated * (scale * scale * scale * along)
    d_mixed = d_gated * z_act
    c = c_ref[...].astype(F32)
    put_pieces(pieces_ref, 0, mm(c * sigmoid(c), d_mixed * wide_ref[...]))
    d_mixed_ref[...] = d_mixed
    grad_z_ref[...] = (d_gated * mixed * (sig * (1.0 + z * (1.0 - sig)))).astype(BF16)


def inside_back_kernel(
    x_ref, b_ref, c_ref, raw_ref, rate_ref, skip_ref, start_ref, wide_ref, d_mixed_ref,
    grad_x_ref, reach_x_ref, reach_s_ref, at_end_ref, d_b_ref, grad_c_ref, small_ref,
    d_scaled_ref,
):
    step, running = clocks(raw_ref[...], rate_ref[...])
    tok, heads = step.shape
    wide = x_ref.shape[1]
    last = running[-1:, :]
    spread = exact(
        jnp.concatenate(
            [step, jnp.exp(last - running), jnp.broadcast_to(skip_ref[...], (8, heads))], axis=0
        ),
        head_lanes(heads, wide),
    )
    step_wide, end_wide = spread[:tok], spread[tok : 2 * tok]
    x = x_ref[...].astype(F32)
    sig = sigmoid(x)
    x_act = x * sig
    scaled = x_act * step_wide
    d_mixed = d_mixed_ref[...]
    b, c = b_ref[...].astype(F32), c_ref[...].astype(F32)
    sig_c = sigmoid(c)
    b_t, c_t = b * sigmoid(b), c * sig_c
    b_act, c_act = b_t.T, c_t.T
    scores, scores_t = mm(c_act, b_t), mm(b_act, c_t)
    running_t = running.T
    rows, cols = iota((tok, tok), 0), iota((tok, tok), 1)
    keep, keep_t = rows >= cols, rows <= cols
    d_scores = jnp.zeros((tok, tok), F32)
    gained = jnp.zeros((tok, heads), F32)
    lost = jnp.zeros((heads, tok), F32)
    head_at, head_row = iota((tok, heads), 1), iota((heads, tok), 0)
    for pair in range(heads // 2):
        lanes = slice(pair * LANES, (pair + 1) * LANES)
        d_parts = halves(d_mixed[:, lanes])
        mixes_t = []
        for half in (0, 1):
            h = 2 * pair + half
            column, row = running[:, h : h + 1], running_t[h : h + 1, :]
            fade = fade_of(column, row, keep)
            mixes_t.append(scores_t * jnp.exp(jnp.where(keep_t, row - column, -1e30)))
            d_fade = mm_nt(d_parts[half], scaled[:, lanes]) * fade
            d_scores = d_scores + d_fade
            flow = d_fade * scores
            gained = jnp.where(head_at == h, jnp.sum(flow, axis=1, keepdims=True), gained)
            lost = jnp.where(head_row == h, jnp.sum(flow, axis=0, keepdims=True), lost)
        d_scaled_ref[:, lanes] = mm(
            jnp.concatenate(mixes_t, axis=1), jnp.concatenate(d_parts, axis=0)
        )
    start = start_ref[...].astype(F32)
    d_carried = d_mixed * wide_ref[...]
    by_head = head_rows(heads, wide)
    d_scaled = d_scaled_ref[...]
    d_run = gained - lost.T + exact(d_carried * mm(c_act, start), by_head)
    d_step = exact(d_scaled * x_act, by_head)
    small_ref[0] = d_run
    small_ref[1] = d_step
    small_ref[2] = jnp.broadcast_to(jnp.exp(last), (tok, heads))
    d_silu = sig * (1.0 + x * (1.0 - sig))
    grad_x_ref[...] = (d_scaled * step_wide + d_mixed * spread[2 * tok : 2 * tok + 1]) * d_silu
    reach_x_ref[...] = end_wide * step_wide * d_silu
    reach_s_ref[...] = end_wide * x_act
    at_end_ref[...] = (scaled * end_wide).astype(BF16)
    d_b_ref[...] = mm(c_t, d_scores)
    d_c = mm_nt(b_t, d_scores) + mm_nt(start, d_carried)
    grad_c_ref[...] = d_c * (sig_c * (1.0 + c * (1.0 - sig_c)))


def leave_kernel(
    pieces_ref, start_ref, b_ref, raw_ref, rate_ref, base_ref, reach_x_ref, reach_s_ref,
    at_end_ref, d_b_ref, small_ref, grad_x_ref, grad_b_ref, grad_step_ref,
):
    after = get_pieces(pieces_ref[...].astype(F32))
    b = b_ref[...].astype(F32)
    sig_b = sigmoid(b)
    reach = mm((b * sig_b).T, after)
    grad_x_ref[...] = (base_ref[...] + reach * reach_x_ref[...]).astype(BF16)
    tok, wide = reach.shape
    raw = raw_ref[...]
    step = softplus(raw).T
    heads = step.shape[1]
    both = jnp.concatenate(
        [
            reach * reach_s_ref[...],
            jnp.broadcast_to(
                jnp.sum(after * start_ref[...].astype(F32), axis=0, keepdims=True), (8, wide)
            ),
        ],
        axis=0,
    )
    sums = exact(both, head_rows(heads, wide))
    lost = step * sums[:tok]
    d_run = small_ref[0] - lost
    end_part = jnp.sum(lost, axis=0, keepdims=True) + small_ref[2][:1] * sums[tok : tok + 1]
    onward = (iota((tok, tok), 0) <= iota((tok, tok), 1)).astype(F32)
    d_log = exact(onward, d_run) + end_part
    d_step = small_ref[1] + sums[:tok] - d_log * rate_ref[...]
    grad_step_ref[...] = d_step.T * sigmoid(raw)
    d_b = d_b_ref[...] + mm_nt(after, at_end_ref[...])
    grad_b_ref[...] = d_b * (sig_b * (1.0 + b * (1.0 - sig_b)))


def local(kernel, name, outs, args, flops, scratch=()):
    return pl.pallas_call(
        kernel,
        out_shape=outs,
        name=name,
        scratch_shapes=scratch,
        cost_estimate=pl.CostEstimate(flops=flops, bytes_accessed=1 << 21, transcendentals=1 << 18),
    )(*args)


def body(
    moe_input,
    cotangent,
    expert_ids,
    routing_weights,
    gate_weight,
    up_weight,
    down_weight,
    inner_x,
    inner_b,
    inner_c,
    gate_z,
    step_raw,
    decay_rate,
    skip_weight,
    norm_gain,
    w_out,
):
    tok = expert_ids.shape[0]
    heads = decay_rate.shape[0]
    experts = lax.axis_size(SP)
    wide = inner_x.shape[1]
    gate_w, up_w, down_w = gate_weight[0], up_weight[0], down_weight[0]
    ids_t, b_t, c_t, raw_t = expert_ids.T, inner_b.T, inner_c.T, step_raw.T
    rate, skip, gain = decay_rate[None, :], skip_weight[None, :], norm_gain[None, :]
    shape = jax.ShapeDtypeStruct

    sent = local(
        enter_kernel,
        "enter",
        shape((experts, 48, LANES), BF16),
        (ids_t, moe_input, inner_x, b_t, raw_t, rate),
        SMALL,
    )
    got_in = to_all(sent, SP)
    weighed = local(
        weigh_kernel,
        "weigh",
        shape((experts, 32, LANES), BF16),
        (ids_t, routing_weights.T, cotangent),
        SMALL,
    )
    sent = local(
        ahead_kernel, "ahead", shape((experts, 40, LANES), BF16), (got_in, weighed), SMALL
    )
    all_in = gathered_x(rows_of(got_in[:, :32]))
    got = to_all(sent, SP)
    all_grad = gathered_x(rows_of(got[:, :32]))

    norm_rows, mixed, start_state, start_wide = local(
        forward_kernel,
        "forward",
        (
            shape((tok, wide), BF16),
            shape((tok, wide), F32),
            shape((STATE, wide), BF16),
            shape((tok, wide), F32),
        ),
        (inner_x, gate_z, b_t, c_t, raw_t, rate, skip, gain, got),
        LARGE,
    )
    norm_y = to_all(jnp.broadcast_to(norm_rows[None], (4, tok, wide)), "y")
    other = lax.ppermute(norm_y, "c", [(0, 1), (1, 0)])
    core = lax.axis_index("c") == 0
    norm_all = jnp.stack([jnp.where(core, norm_y, other), jnp.where(core, other, norm_y)], axis=1)

    gate_w4 = gate_w.reshape(4, -1, gate_w.shape[1])
    up_w4 = up_w.reshape(4, -1, up_w.shape[1])
    gate_pre = jnp.einsum("krd,kdf->rf", all_in, gate_w4, preferred_element_type=F32)
    up_pre = jnp.einsum("krd,kdf->rf", all_in, up_w4, preferred_element_type=F32)
    down_w4 = down_w.reshape(down_w.shape[0], 4, -1)
    hidden_grad = jnp.einsum("krd,fkd->rf", all_grad, down_w4, preferred_element_type=F32)
    sig_gate = jax.nn.sigmoid(gate_pre)
    active = gate_pre * sig_gate
    hidden = (active * up_pre).astype(BF16)
    gate_grad = (hidden_grad * up_pre * sig_gate * (1.0 + gate_pre * (1.0 - sig_gate))).astype(BF16)
    up_grad = (hidden_grad * active).astype(BF16)
    terms = jnp.einsum("rf,kdf->krd", gate_grad, gate_w4, preferred_element_type=F32)
    terms = terms + jnp.einsum("rf,kdf->krd", up_grad, up_w4, preferred_element_type=F32)
    slot_grad = summed_x(terms.astype(BF16))
    back = to_all(slot_grad.reshape(experts, SLOTS, -1), SP).reshape(experts * SLOTS, -1)
    gate_out = jnp.einsum("krd,rf->kdf", all_in, gate_grad, preferred_element_type=F32)
    up_out = jnp.einsum("krd,rf->kdf", all_in, up_grad, preferred_element_type=F32)
    down_out = jnp.einsum("rf,krd->fkd", hidden, all_grad, preferred_element_type=F32)

    mixer_cols = local(
        combine_kernel,
        "combine",
        shape((4, *cotangent.shape), BF16),
        (ids_t, cotangent, back),
        SMALL,
    )
    mixer4 = to_all(mixer_cols, "x")
    w_out4 = w_out.reshape(4, -1, wide)
    norm_grad = jnp.einsum("ktd,kdn->tn", mixer4, w_out4, preferred_element_type=F32)

    mixer_t = mixer4.transpose(0, 2, 1).reshape(8, 8, 32, tok).transpose(1, 0, 2, 3)
    mixer_t = to_all(mixer_t, ("y", "c"))

    pieces, grad_z, d_mixed = local(
        gate_back_kernel,
        "gate_back",
        (
            shape((experts, 8, LANES), BF16),
            shape((tok, wide), BF16),
            shape((tok, wide), F32),
        ),
        (norm_grad, mixed, gate_z, gain, start_wide, c_t),
        SMALL,
    )
    pieces = to_all(pieces, SP)
    partial = jnp.einsum(
        "kzrt,ktn->zrn",
        mixer_t,
        norm_all.reshape(8, tok, wide),
        preferred_element_type=F32,
    ).astype(BF16)
    grad_out = jnp.sum(to_all(partial, "z").astype(F32), axis=0)
    pieces = local(
        behind_kernel, "behind", shape((experts, 8, LANES), BF16), (got_in, pieces), SMALL
    )
    pieces = to_all(pieces, SP)
    grad_x, reach_x, reach_s, at_end, d_b, grad_c, small = local(
        inside_back_kernel,
        "inside_back",
        (
            shape((tok, wide), F32),
            shape((tok, wide), F32),
            shape((tok, wide), F32),
            shape((tok, wide), BF16),
            shape((STATE, tok), F32),
            shape((STATE, tok), F32),
            shape((3, tok, heads), F32),
        ),
        (inner_x, b_t, c_t, raw_t, rate, skip, start_state, start_wide, d_mixed),
        LARGE,
        (pltpu.VMEM((tok, wide), F32),),
    )
    grad_x, grad_b, grad_step = local(
        leave_kernel,
        "leave",
        (shape((tok, wide), BF16), shape((STATE, tok), F32), shape((heads, tok), F32)),
        (pieces, start_state, b_t, raw_t, rate, grad_x, reach_x, reach_s, at_end, d_b, small),
        SMALL,
    )
    return (
        gate_out.reshape(gate_weight.shape).astype(BF16),
        up_out.reshape(up_weight.shape).astype(BF16),
        down_out.reshape(down_weight.shape).astype(BF16),
        grad_out,
        grad_x,
        grad_b.T,
        grad_c.T,
        grad_z,
        grad_step.T,
    )


def solution(mesh):
    finer = Mesh(mesh.devices.reshape(8, 4, 2, mesh.shape["tp"]), ("z", "y", "c", "x"))
    return jax.shard_map(
        body,
        mesh=finer,
        in_specs=(
            P(SP, "x"),
            P(SP, "x"),
            P(SP, None),
            P(SP, None),
            P(SP, None, "x"),
            P(SP, None, "x"),
            P(SP, "x", None),
            P(SP, "x"),
            P(SP, "x"),
            P(SP, "x"),
            P(SP, "x"),
            P(SP, "x"),
            P("x"),
            P("x"),
            P("x"),
            P(None, "x"),
        ),
        out_specs=(
            P(SP, None, "x"),
            P(SP, None, "x"),
            P(SP, "x", None),
            P(SP, "x"),
            P(SP, "x"),
            P(SP, "x"),
            P(SP, "x"),
            P(SP, "x"),
            P(SP, "x"),
        ),
        check_vma=False,
    )
```

```python
import jax
import jax.numpy as jnp
from jax import lax
from jax.sharding import Mesh
from jax.experimental import pallas as pl
from jax.experimental.pallas import tpu as pltpu
from jax.sharding import PartitionSpec as P

HEAD_DIM = 64
STATE = 64
LANES = 128
SLOTS = 8
EPS = 0.01
SP = ("z", "y", "c")
F32 = jnp.float32
BF16 = jnp.bfloat16
HIGH = lax.Precision.HIGHEST


def along(value, axis, step):
    count = lax.axis_size(axis)
    return lax.ppermute(value, axis, [(i, (i + step) % count) for i in range(count)])


def shifted(value, step):
    return along(value, "x", step)


def to_all(value, axes):
    return lax.all_to_all(value, axes, split_axis=0, concat_axis=0, tiled=True)


def relayed(left, right):
    half = left.shape[0] // 2
    return jnp.concatenate([shifted(left[:half], 1), shifted(right[half:], -1)], axis=0)


def summed_x(far, far2, up1, up2, down1, down2, rest):
    half = far.shape[0]
    from_left, from_right = shifted(far, 1), shifted(far2, -1)
    low2, high1 = shifted(up2, 1), shifted(down1, -1)
    up1 = (up1.astype(F32) + from_left.astype(F32)).astype(BF16)
    down2 = (down2.astype(F32) + from_right.astype(F32)).astype(BF16)
    low1, high2 = shifted(up1, 1), shifted(down2, -1)
    rest = rest.astype(F32)
    first = rest[:half] + low1.astype(F32) + high1.astype(F32)
    second = rest[half:] + low2.astype(F32) + high2.astype(F32)
    return jnp.concatenate([first, second], axis=0).astype(BF16)


def rows_of(tiled):
    cols = tiled.shape[1] // SLOTS
    rows = tiled.reshape(-1, cols, SLOTS, LANES).transpose(0, 2, 1, 3)
    return rows.reshape(-1, cols * LANES)


SMALL, LARGE = 1 << 30, 1 << 32


def softplus(value):
    small = jnp.exp(-jnp.abs(value))
    grown = 1.0 + small
    log_part = jnp.where(
        grown == 1.0, small, jnp.log(grown) * (small / jnp.where(grown == 1.0, 1.0, grown - 1.0))
    )
    return jnp.maximum(value, 0.0) + log_part


def sigmoid(value):
    return 1.0 / (1.0 + jnp.exp(-value))


def mm(left, right):
    return jnp.dot(left.astype(BF16), right.astype(BF16), preferred_element_type=F32)


def mm_nt(left, right):
    return lax.dot_general(
        left.astype(BF16),
        right.astype(BF16),
        (((1,), (1,)), ((), ())),
        preferred_element_type=F32,
    )


def exact(left, right):
    return jnp.dot(left, right, preferred_element_type=F32, precision=HIGH)


def iota(shape, dim):
    return lax.broadcasted_iota(jnp.int32, shape, dim)


def head_lanes(heads, wide):
    return ((iota((heads, wide), 1) >> 6) == iota((heads, wide), 0)).astype(F32)


def head_rows(heads, wide):
    return ((iota((wide, heads), 0) >> 6) == iota((wide, heads), 1)).astype(F32)


def clocks(raw_t, rate):
    step = softplus(raw_t).T
    logs = -step * rate
    tok = logs.shape[0]
    upto = (iota((tok, tok), 0) >= iota((tok, tok), 1)).astype(F32)
    return step, exact(upto, logs)


def routing(ids_t, experts):
    numbers = iota((experts, ids_t.shape[1]), 0)
    first, second = ids_t[0:1, :] == numbers, ids_t[1:2, :] == numbers
    named = jnp.where(first, 1.0, jnp.where(second, 1.0, 0.0))
    tok = ids_t.shape[1]
    earlier = (iota((tok, tok), 0) < iota((tok, tok), 1)).astype(F32)
    before = mm(named, earlier)
    key = jnp.where(named > 0.0, before, -1.0)
    shape = (experts, SLOTS, tok)
    pick = jnp.broadcast_to(key[:, None, :], shape) == iota(shape, 1).astype(F32)
    return first, second, jnp.where(pick, 1.0, 0.0)


def put_tiles(out_ref, rows, experts):
    cols = rows.shape[1] // LANES
    tiled = rows.reshape(experts, SLOTS, rows.shape[1])
    for col in range(cols):
        out_ref[:, col * SLOTS : (col + 1) * SLOTS, :] = tiled[
            :, :, col * LANES : (col + 1) * LANES
        ].astype(BF16)


def put_pieces(out_ref, at, state):
    rows = state.shape[0] // 8
    for col in range(state.shape[1] // LANES):
        piece = state[:, col * LANES : (col + 1) * LANES].reshape(rows, 8, LANES)
        out_ref[col * rows : (col + 1) * rows, at : at + 8, :] = piece.astype(BF16)


def get_pieces(pieces):
    rows = STATE // 8
    cols = pieces.shape[0] // rows
    return jnp.concatenate(
        [pieces[col * rows : (col + 1) * rows].reshape(STATE, LANES) for col in range(cols)],
        axis=1,
    )


def enter_kernel(ids_ref, moe_ref, out_ref):
    experts = out_ref.shape[0]
    pick = routing(ids_ref[...], experts)[2]
    put_tiles(out_ref, mm(pick.reshape(experts * SLOTS, -1), moe_ref[...]), experts)


def put_fresh(x_ref, b_ref, raw_ref, rate_ref, out_ref):
    step, running = clocks(raw_ref[...], rate_ref[...])
    heads, wide = step.shape[1], x_ref.shape[1]
    last = running[-1:, :]
    spread = exact(
        jnp.concatenate(
            [step * jnp.exp(last - running), jnp.broadcast_to(jnp.exp(last), (8, heads))], axis=0
        ),
        head_lanes(heads, wide),
    )
    x = x_ref[...].astype(F32)
    at_end = x * sigmoid(x) * spread[:-8]
    b = b_ref[...].astype(F32)
    put_pieces(out_ref, 32, mm(b * sigmoid(b), at_end))
    total = spread[-8:]
    high = total.astype(BF16).astype(F32)
    mid = (total - high).astype(BF16).astype(F32)
    low = total - high - mid
    row = iota(total.shape, 0)
    tile = jnp.where(row == 0, high, jnp.where(row == 1, mid, jnp.where(row == 2, low, 0.0)))
    rows_at = STATE // 8
    for col in range(wide // LANES):
        part = tile[:, col * LANES : (col + 1) * LANES].astype(BF16)
        out_ref[col * rows_at : (col + 1) * rows_at, 40:48, :] = jnp.broadcast_to(
            part[None], (rows_at, 8, LANES)
        )


def weigh_kernel(ids_ref, weights_ref, cot_ref, x_ref, b_ref, raw_ref, rate_ref, out_ref):
    put_fresh(x_ref, b_ref, raw_ref, rate_ref, out_ref)
    experts = out_ref.shape[0]
    first, second, pick = routing(ids_ref[...], experts)
    weights = weights_ref[...]
    weight_at = jnp.where(first, weights[0:1, :], 0.0) + jnp.where(second, weights[1:2, :], 0.0)
    scaling = jnp.sum(
        pick * jnp.broadcast_to(weight_at[:, None, :], pick.shape), axis=2, keepdims=True
    )
    rows = mm(pick.reshape(experts * SLOTS, -1), cot_ref[...])
    put_tiles(
        out_ref,
        (rows.reshape(experts, SLOTS, -1) * scaling).reshape(experts * SLOTS, -1),
        experts,
    )


def block_decays(got_ref):
    tile = got_ref[:, 40:48, :].astype(F32)
    total = tile[:, 0:1, :] + tile[:, 1:2, :] + tile[:, 2:3, :]
    return jnp.broadcast_to(total, tile.shape)


def ahead_kernel(got_ref, out_ref):
    decays = block_decays(got_ref)
    pieces = got_ref[:, 32:40, :].astype(F32)
    total = jnp.zeros(pieces.shape[1:], F32)
    found = []
    for k in range(pieces.shape[0]):
        found.append(total)
        total = total * decays[k] + pieces[k]
    out_ref[...] = jnp.stack(found, axis=0).astype(BF16)


def behind_kernel(got_ref, pieces_ref, out_ref):
    decays = block_decays(got_ref)
    pieces = pieces_ref[...].astype(F32)
    total = jnp.zeros(pieces.shape[1:], F32)
    found = []
    for k in reversed(range(pieces.shape[0])):
        found.append(total)
        total = total * decays[k] + pieces[k]
    out_ref[...] = jnp.stack(found[::-1], axis=0).astype(BF16)


def first_kernel(here_ref, own_ref, left_ref, right_ref, far_ref, gate_ref, up_ref, out_gate_ref, out_up_ref):
    here = here_ref[0]
    for weight_ref, out_ref in ((gate_ref, out_gate_ref), (up_ref, out_up_ref)):
        total = None
        for block_ref, offset in ((own_ref, 0), (left_ref, 3), (right_ref, 1), (far_ref, 2)):
            width = block_ref.shape[1]
            at = pl.multiple_of(((here + offset) & 3) * width, width)
            term = mm(block_ref[...], weight_ref[pl.ds(at, width), :])
            total = term if total is None else total + term
        out_ref[...] = total


def middle_kernel(
    here_ref, own_ref, left_ref, right_ref, op_ref, down_ref, pre_ref, up_pre_ref, gate_ref, up_ref,
    hidden_ref, gate_grad_ref, up_grad_ref, far_ref, far2_ref, up1_ref, up2_ref, down1_ref, down2_ref,
    rest_ref,
):
    here = here_ref[0]
    hidden_grad = None
    for block_ref, offset in ((own_ref, 0), (left_ref, 3), (right_ref, 1), (op_ref, 2)):
        width = block_ref.shape[1]
        at = pl.multiple_of(((here + offset) & 3) * width, width)
        term = mm_nt(block_ref[...], down_ref[:, pl.ds(at, width)])
        hidden_grad = term if hidden_grad is None else hidden_grad + term
    pre, up_pre = pre_ref[...], up_pre_ref[...]
    sig = sigmoid(pre)
    active = pre * sig
    hidden_ref[...] = (active * up_pre).astype(BF16)
    gate_grad = (hidden_grad * up_pre * sig * (1.0 + pre * (1.0 - sig))).astype(BF16)
    up_grad = (hidden_grad * active).astype(BF16)
    gate_grad_ref[...] = gate_grad
    up_grad_ref[...] = up_grad
    width = rest_ref.shape[1]
    half = rest_ref.shape[0] // 2
    for offset, low_ref, high_ref in (
        (2, far_ref, far2_ref), (1, up1_ref, up2_ref), (3, down1_ref, down2_ref), (0, None, None)
    ):
        at = pl.multiple_of(((here + offset) & 3) * width, width)
        term = mm_nt(gate_grad, gate_ref[pl.ds(at, width), :]) + mm_nt(
            up_grad, up_ref[pl.ds(at, width), :]
        )
        term = term.astype(BF16)
        if low_ref is None:
            rest_ref[...] = term
        else:
            low_ref[...] = term[:half]
            high_ref[...] = term[half:]


def weights_kernel(
    here_ref, in0_ref, in1_ref, in2_ref, in3_ref, out0_ref, out1_ref, out2_ref, out3_ref,
    hidden_ref, gate_grad_ref, up_grad_ref, gate_ref, up_ref, down_ref,
):
    here = here_ref[0]
    hidden_t = hidden_ref[...].T
    for in_ref, grad_ref, offset in (
        (in0_ref, out0_ref, 0), (in1_ref, out1_ref, 3), (in2_ref, out2_ref, 1), (in3_ref, out3_ref, 2)
    ):
        width = in_ref.shape[1]
        at = pl.multiple_of(((here + offset) & 3) * width, width)
        block_t = in_ref[...].T
        gate_ref[pl.ds(at, width), :] = mm(block_t, gate_grad_ref[...]).astype(BF16)
        up_ref[pl.ds(at, width), :] = mm(block_t, up_grad_ref[...]).astype(BF16)
        down_ref[:, pl.ds(at, width)] = mm(hidden_t, grad_ref[...]).astype(BF16)


def combine_kernel(ids_ref, cot_ref, back_ref, out_ref):
    experts = back_ref.shape[0] // SLOTS
    pick = routing(ids_ref[...], experts)[2].reshape(experts * SLOTS, -1)
    moe_grad = mm(pick.T, back_ref[...])
    rows = (cot_ref[...].astype(F32) + moe_grad).astype(BF16)
    for k in range(out_ref.shape[0]):
        out_ref[k] = rows


def halves(value):
    low = iota(value.shape, 1) < HEAD_DIM
    return jnp.where(low, value, 0.0), jnp.where(low, 0.0, value)


def fade_of(column, row, keep):
    return jnp.exp(jnp.where(keep, column - row, -1e30))


def forward_kernel(
    x_ref, z_ref, b_ref, c_ref, raw_ref, rate_ref, skip_ref, gain_ref, got_ref,
    norm_ref, mixed_ref, start_ref, wide_ref,
):
    start = get_pieces(got_ref[...].astype(F32))
    start_ref[...] = start.astype(BF16)
    step, running = clocks(raw_ref[...], rate_ref[...])
    tok, heads = step.shape
    wide = x_ref.shape[1]
    spread = exact(
        jnp.concatenate(
            [step, jnp.exp(running), jnp.broadcast_to(skip_ref[...], (8, heads))], axis=0
        ),
        head_lanes(heads, wide),
    )
    x = x_ref[...].astype(F32)
    x_act = x * sigmoid(x)
    scaled = x_act * spread[:tok]
    wide_ref[...] = spread[tok : 2 * tok]
    b, c = b_ref[...].astype(F32), c_ref[...].astype(F32)
    b_t, c_t = b * sigmoid(b), c * sigmoid(c)
    c_act = c_t.T
    scores = mm(c_act, b_t)
    mixed = spread[tok : 2 * tok] * mm(c_act, start) + x_act * spread[2 * tok : 2 * tok + 1]
    running_t = running.T
    keep = iota((tok, tok), 0) >= iota((tok, tok), 1)
    for pair in range(heads // 2):
        lanes = slice(pair * LANES, (pair + 1) * LANES)
        mixes = [
            scores * fade_of(running[:, h : h + 1], running_t[h : h + 1, :], keep)
            for h in (2 * pair, 2 * pair + 1)
        ]
        inside = mm(
            jnp.concatenate(mixes, axis=1), jnp.concatenate(halves(scaled[:, lanes]), axis=0)
        )
        mixed_ref[:, lanes] = mixed[:, lanes] + inside
    z = z_ref[...].astype(F32)
    gated = mixed_ref[...] * (z * sigmoid(z))
    scale = lax.rsqrt(jnp.mean(gated * gated, axis=1, keepdims=True) + EPS)
    norm_ref[...] = (gated * scale * gain_ref[...]).astype(BF16)


def gate_back_kernel(
    rows_ref, w_ref, mixed_ref, z_ref, gain_ref, wide_ref, c_ref, pieces_ref, grad_z_ref, d_mixed_ref
):
    z = z_ref[...].astype(F32)
    sig = sigmoid(z)
    z_act = z * sig
    mixed = mixed_ref[...]
    gated = mixed * z_act
    scale = lax.rsqrt(jnp.mean(gated * gated, axis=1, keepdims=True) + EPS)
    rows = jnp.concatenate([rows_ref[k] for k in range(rows_ref.shape[0])], axis=1)
    d_norm = mm(rows, w_ref[...]) * gain_ref[...]
    along_row = jnp.mean(d_norm * gated, axis=1, keepdims=True)
    d_gated = scale * d_norm - gated * (scale * scale * scale * along_row)
    d_mixed = d_gated * z_act
    c = c_ref[...].astype(F32)
    put_pieces(pieces_ref, 0, mm(c * sigmoid(c), d_mixed * wide_ref[...]))
    d_mixed_ref[...] = d_mixed
    grad_z_ref[...] = (d_gated * mixed * (sig * (1.0 + z * (1.0 - sig)))).astype(BF16)


def project_kernel(*refs):
    plane = refs[0][0]
    part_refs, near_refs, far_refs = refs[1:5], refs[5:9], refs[9:13]
    own_ref, share_refs, left_ref = refs[13], refs[14:21], refs[21]
    tok = near_refs[0].shape[0]
    planes, rows = part_refs[0].shape[1], part_refs[0].shape[2]
    for step in range(planes):
        for k, part_ref in enumerate(part_refs):
            for half in (0, 1):
                at = (2 * k + half) * tok
                left_ref[step * rows : (step + 1) * rows, at : at + tok] = part_ref[
                    half, (plane + step) & (planes - 1)
                ]
    total = None
    for k in range(4):
        for half, block_ref in enumerate((near_refs[k], far_refs[k])):
            at = (2 * k + half) * tok
            term = mm(left_ref[:, at : at + tok], block_ref[...])
            total = term if total is None else total + term
    own_ref[...] = total[:rows]
    for step in range(1, planes):
        share_refs[step - 1][...] = total[step * rows : (step + 1) * rows].astype(BF16)


def inside_back_kernel(
    x_ref, b_ref, c_ref, raw_ref, rate_ref, skip_ref, start_ref, wide_ref, d_mixed_ref,
    grad_x_ref, reach_x_ref, reach_s_ref, at_end_ref, d_b_ref, grad_c_ref, small_ref,
    d_scaled_ref,
):
    step, running = clocks(raw_ref[...], rate_ref[...])
    tok, heads = step.shape
    wide = x_ref.shape[1]
    last = running[-1:, :]
    spread = exact(
        jnp.concatenate(
            [step, jnp.exp(last - running), jnp.broadcast_to(skip_ref[...], (8, heads))], axis=0
        ),
        head_lanes(heads, wide),
    )
    step_wide, end_wide = spread[:tok], spread[tok : 2 * tok]
    x = x_ref[...].astype(F32)
    sig = sigmoid(x)
    x_act = x * sig
    scaled = x_act * step_wide
    d_mixed = d_mixed_ref[...]
    b, c = b_ref[...].astype(F32), c_ref[...].astype(F32)
    sig_c = sigmoid(c)
    b_t, c_t = b * sigmoid(b), c * sig_c
    b_act, c_act = b_t.T, c_t.T
    scores, scores_t = mm(c_act, b_t), mm(b_act, c_t)
    running_t = running.T
    rows, cols = iota((tok, tok), 0), iota((tok, tok), 1)
    keep, keep_t = rows >= cols, rows <= cols
    d_scores = jnp.zeros((tok, tok), F32)
    gained = jnp.zeros((tok, heads), F32)
    lost = jnp.zeros((heads, tok), F32)
    head_at, head_row = iota((tok, heads), 1), iota((heads, tok), 0)
    for pair in range(heads // 2):
        lanes = slice(pair * LANES, (pair + 1) * LANES)
        d_parts = halves(d_mixed[:, lanes])
        mixes_t = []
        for half in (0, 1):
            h = 2 * pair + half
            column, row = running[:, h : h + 1], running_t[h : h + 1, :]
            fade = fade_of(column, row, keep)
            mixes_t.append(scores_t * jnp.exp(jnp.where(keep_t, row - column, -1e30)))
            d_fade = mm_nt(d_parts[half], scaled[:, lanes]) * fade
            d_scores = d_scores + d_fade
            flow = d_fade * scores
            gained = jnp.where(head_at == h, jnp.sum(flow, axis=1, keepdims=True), gained)
            lost = jnp.where(head_row == h, jnp.sum(flow, axis=0, keepdims=True), lost)
        d_scaled_ref[:, lanes] = mm(
            jnp.concatenate(mixes_t, axis=1), jnp.concatenate(d_parts, axis=0)
        )
    start = start_ref[...].astype(F32)
    d_carried = d_mixed * wide_ref[...]
    by_head = head_rows(heads, wide)
    d_scaled = d_scaled_ref[...]
    d_run = gained - lost.T + exact(d_carried * mm(c_act, start), by_head)
    d_step = exact(d_scaled * x_act, by_head)
    small_ref[0] = d_run
    small_ref[1] = d_step
    small_ref[2] = jnp.broadcast_to(jnp.exp(last), (tok, heads))
    d_silu = sig * (1.0 + x * (1.0 - sig))
    grad_x_ref[...] = (d_scaled * step_wide + d_mixed * spread[2 * tok : 2 * tok + 1]) * d_silu
    reach_x_ref[...] = end_wide * step_wide * d_silu
    reach_s_ref[...] = end_wide * x_act
    at_end_ref[...] = (scaled * end_wide).astype(BF16)
    d_b_ref[...] = mm(c_t, d_scores)
    d_c = mm_nt(b_t, d_scores) + mm_nt(start, d_carried)
    grad_c_ref[...] = d_c * (sig_c * (1.0 + c * (1.0 - sig_c)))


def leave_kernel(
    pieces_ref, start_ref, b_ref, raw_ref, rate_ref, base_ref, reach_x_ref, reach_s_ref,
    at_end_ref, d_b_ref, small_ref, grad_x_ref, grad_b_ref, grad_step_ref,
):
    after = get_pieces(pieces_ref[...].astype(F32))
    b = b_ref[...].astype(F32)
    sig_b = sigmoid(b)
    reach = mm((b * sig_b).T, after)
    grad_x_ref[...] = (base_ref[...] + reach * reach_x_ref[...]).astype(BF16)
    tok, wide = reach.shape
    raw = raw_ref[...]
    step = softplus(raw).T
    heads = step.shape[1]
    both = jnp.concatenate(
        [
            reach * reach_s_ref[...],
            jnp.broadcast_to(
                jnp.sum(after * start_ref[...].astype(F32), axis=0, keepdims=True), (8, wide)
            ),
        ],
        axis=0,
    )
    sums = exact(both, head_rows(heads, wide))
    lost = step * sums[:tok]
    d_run = small_ref[0] - lost
    end_part = jnp.sum(lost, axis=0, keepdims=True) + small_ref[2][:1] * sums[tok : tok + 1]
    onward = (iota((tok, tok), 0) <= iota((tok, tok), 1)).astype(F32)
    d_log = exact(onward, d_run) + end_part
    d_step = small_ref[1] + sums[:tok] - d_log * rate_ref[...]
    grad_step_ref[...] = d_step.T * sigmoid(raw)
    d_b = d_b_ref[...] + mm_nt(after, at_end_ref[...])
    grad_b_ref[...] = d_b * (sig_b * (1.0 + b * (1.0 - sig_b)))


def local(kernel, outs, args, flops, scratch=(), scalars=0):
    specs = [pl.BlockSpec(memory_space=pltpu.SMEM)] * scalars + [
        pl.BlockSpec(memory_space=pltpu.VMEM)
    ] * (len(args) - scalars)
    return pl.pallas_call(
        kernel,
        out_shape=outs,
        scratch_shapes=scratch,
        in_specs=specs,
        compiler_params=pltpu.CompilerParams(vmem_limit_bytes=16 << 20),
        cost_estimate=pl.CostEstimate(flops=flops, bytes_accessed=1 << 21, transcendentals=1 << 18),
    )(*args)


def body(
    moe_input,
    cotangent,
    expert_ids,
    routing_weights,
    gate_weight,
    up_weight,
    down_weight,
    inner_x,
    inner_b,
    inner_c,
    gate_z,
    step_raw,
    decay_rate,
    skip_weight,
    norm_gain,
    w_out,
):
    tok = expert_ids.shape[0]
    heads = decay_rate.shape[0]
    experts = lax.axis_size(SP)
    wide = inner_x.shape[1]
    gate_w, up_w, down_w = gate_weight[0], up_weight[0], down_weight[0]
    ids_t, b_t, c_t, raw_t = expert_ids.T, inner_b.T, inner_c.T, step_raw.T
    rate, skip, gain = decay_rate[None, :], skip_weight[None, :], norm_gain[None, :]
    here = lax.axis_index("x")[None]
    shape = jax.ShapeDtypeStruct
    slots = experts * SLOTS
    cols, inner = moe_input.shape[1], gate_w.shape[1]

    sent_in = local(enter_kernel, shape((experts, 32, LANES), BF16), (ids_t, moe_input), SMALL)
    got_in = to_all(sent_in, SP)
    sent_grad = local(
        weigh_kernel,
        shape((experts, 48, LANES), BF16),
        (ids_t, routing_weights.T, cotangent, inner_x, b_t, raw_t, rate),
        SMALL,
    )
    got_grad = to_all(sent_grad, SP)

    rows_in = rows_of(got_in)
    in_left, in_right = shifted(rows_in, 1), shifted(rows_in, -1)
    in_far = relayed(in_left, in_right)
    pre, up_pre = local(
        first_kernel,
        (shape((slots, inner), F32), shape((slots, inner), F32)),
        (here, rows_in, in_left, in_right, in_far, gate_w, up_w),
        SMALL,
        scalars=1,
    )
    rows_grad = rows_of(got_grad[:, :32])
    grad_left, grad_right = shifted(rows_grad, 1), shifted(rows_grad, -1)
    grad_far = relayed(grad_left, grad_right)

    pieces = local(ahead_kernel, shape((experts, 8, LANES), BF16), (got_grad,), SMALL)
    pieces = to_all(pieces, SP)

    hidden, gate_grad, up_grad, *terms = local(
        middle_kernel,
        (
            shape((slots, inner), BF16),
            shape((slots, inner), BF16),
            shape((slots, inner), BF16),
            *[shape((slots // 2, cols), BF16)] * 6,
            shape((slots, cols), BF16),
        ),
        (here, rows_grad, grad_left, grad_right, grad_far, down_w, pre, up_pre, gate_w, up_w),
        SMALL,
        scalars=1,
    )
    slot_grad = summed_x(*terms)

    norm_rows, mixed, start_state, start_wide = local(
        forward_kernel,
        (
            shape((tok, wide), BF16),
            shape((tok, wide), F32),
            shape((STATE, wide), BF16),
            shape((tok, wide), F32),
        ),
        (inner_x, gate_z, b_t, c_t, raw_t, rate, skip, gain, pieces),
        SMALL,
    )
    slot_grad, norm_rows, mixed, start_wide = lax.optimization_barrier(
        (slot_grad, norm_rows, mixed, start_wide)
    )
    norm_y = [norm_rows] + [along(norm_rows, "y", step) for step in (1, 2, 3)]
    back = to_all(slot_grad.reshape(experts, SLOTS, -1), SP).reshape(slots, -1)
    norm_c = [along(rows, "c", 1) for rows in norm_y]
    gate_out, up_out, down_out = local(
        weights_kernel,
        (
            shape(gate_w.shape, BF16),
            shape(up_w.shape, BF16),
            shape(down_w.shape, BF16),
        ),
        (
            here, rows_in, in_left, in_right, in_far, rows_grad, grad_left, grad_right, grad_far,
            hidden, gate_grad, up_grad,
        ),
        LARGE,
        scalars=1,
    )
    back, gate_out, up_out, down_out, norm_c = lax.optimization_barrier(
        (back, gate_out, up_out, down_out, norm_c)
    )

    mixer_cols = local(
        combine_kernel, shape((4, *cotangent.shape), BF16), (ids_t, cotangent, back), SMALL
    )
    mixer4 = to_all(mixer_cols, "x")

    pieces, grad_z, d_mixed = local(
        gate_back_kernel,
        (
            shape((experts, 8, LANES), BF16),
            shape((tok, wide), BF16),
            shape((tok, wide), F32),
        ),
        (mixer4, w_out, mixed, gate_z, gain, start_wide, c_t),
        SMALL,
    )

    mine, row, plane = lax.axis_index("c"), lax.axis_index("y"), lax.axis_index("z")
    mixer_t = mixer4.transpose(0, 2, 1).reshape(8, 4, 2, 32, tok).transpose(2, 1, 0, 3, 4)
    pieces, mixer_t = lax.optimization_barrier((pieces, mixer_t))
    pieces = to_all(pieces, SP)
    keep = lax.dynamic_index_in_dim(mixer_t, mine, 0, keepdims=False)
    give = lax.dynamic_index_in_dim(mixer_t, 1 - mine, 0, keepdims=False)
    take = along(give, "c", 1)
    both = jnp.stack([keep, take], axis=0)
    parts = [lax.dynamic_index_in_dim(both, row, 1, keepdims=False)] + [
        along(
            lax.dynamic_index_in_dim(both, (row + step) % 4, 1, keepdims=False), "y", step
        )
        for step in (1, 2, 3)
    ]
    found = local(
        project_kernel,
        (shape((32, wide), F32), *[shape((32, wide), BF16)] * 7),
        (plane[None], *parts, *norm_y, *norm_c),
        SMALL,
        (pltpu.VMEM((256, 8 * tok), BF16),),
        scalars=1,
    )
    grad_out = found[0]
    for step in (4, 3, 5, 2, 6, 1, 7):
        grad_out = grad_out + along(found[step], "z", step).astype(F32)
    pieces = local(behind_kernel, shape((experts, 8, LANES), BF16), (got_grad, pieces), SMALL)
    pieces = to_all(pieces, SP)
    grad_x, reach_x, reach_s, at_end, d_b, grad_c, small = local(
        inside_back_kernel,
        (
            shape((tok, wide), F32),
            shape((tok, wide), F32),
            shape((tok, wide), F32),
            shape((tok, wide), BF16),
            shape((STATE, tok), F32),
            shape((STATE, tok), F32),
            shape((3, tok, heads), F32),
        ),
        (inner_x, b_t, c_t, raw_t, rate, skip, start_state, start_wide, d_mixed),
        LARGE,
        (pltpu.VMEM((tok, wide), F32),),
    )
    grad_x, grad_b, grad_step = local(
        leave_kernel,
        (shape((tok, wide), BF16), shape((STATE, tok), F32), shape((heads, tok), F32)),
        (pieces, start_state, b_t, raw_t, rate, grad_x, reach_x, reach_s, at_end, d_b, small),
        SMALL,
    )
    return (
        gate_out[None],
        up_out[None],
        down_out[None],
        grad_out,
        grad_x,
        grad_b.T,
        grad_c.T,
        grad_z,
        grad_step.T,
    )


def solution(mesh):
    finer = Mesh(mesh.devices.reshape(8, 4, 2, mesh.shape["tp"]), ("z", "y", "c", "x"))
    return jax.shard_map(
        body,
        mesh=finer,
        in_specs=(
            P(SP, "x"),
            P(SP, "x"),
            P(SP, None),
            P(SP, None),
            P(SP, None, "x"),
            P(SP, None, "x"),
            P(SP, "x", None),
            P(SP, "x"),
            P(SP, "x"),
            P(SP, "x"),
            P(SP, "x"),
            P(SP, "x"),
            P("x"),
            P("x"),
            P("x"),
            P(None, "x"),
        ),
        out_specs=(
            P(SP, None, "x"),
            P(SP, None, "x"),
            P(SP, "x", None),
            P(SP, "x"),
            P(SP, "x"),
            P(SP, "x"),
            P(SP, "x"),
            P(SP, "x"),
            P(SP, "x"),
        ),
        check_vma=False,
    )
```

```python
import jax
import jax.numpy as jnp
from jax import lax
from jax.sharding import Mesh
from jax.experimental import pallas as pl
from jax.experimental.pallas import tpu as pltpu
from jax.sharding import PartitionSpec as P

HEAD_DIM = 64
STATE = 64
LANES = 128
SLOTS = 8
EPS = 0.01
SP = ("z", "y", "c")
F32 = jnp.float32
BF16 = jnp.bfloat16
HIGH = lax.Precision.HIGHEST


def along(value, axis, step):
    count = lax.axis_size(axis)
    return lax.ppermute(value, axis, [(i, (i + step) % count) for i in range(count)])


def shifted(value, step):
    return along(value, "x", step)


def to_all(value, axes):
    return lax.all_to_all(value, axes, split_axis=0, concat_axis=0, tiled=True)


def around(value):
    return shifted(value, 1), shifted(value, -1), shifted(value, 2)


def rows_of(tiled):
    cols = tiled.shape[1] // SLOTS
    rows = tiled.reshape(-1, cols, SLOTS, LANES).transpose(0, 2, 1, 3)
    return rows.reshape(-1, cols * LANES)


SMALL, LARGE = 1 << 30, 1 << 32


def softplus(value):
    small = jnp.exp(-jnp.abs(value))
    grown = 1.0 + small
    log_part = jnp.where(
        grown == 1.0, small, jnp.log(grown) * (small / jnp.where(grown == 1.0, 1.0, grown - 1.0))
    )
    return jnp.maximum(value, 0.0) + log_part


def sigmoid(value):
    return 1.0 / (1.0 + jnp.exp(-value))


def mm(left, right):
    return jnp.dot(left.astype(BF16), right.astype(BF16), preferred_element_type=F32)


def mm_nt(left, right):
    return lax.dot_general(
        left.astype(BF16),
        right.astype(BF16),
        (((1,), (1,)), ((), ())),
        preferred_element_type=F32,
    )


def exact(left, right):
    return jnp.dot(left, right, preferred_element_type=F32, precision=HIGH)


def iota(shape, dim):
    return lax.broadcasted_iota(jnp.int32, shape, dim)


def head_lanes(heads, wide):
    return ((iota((heads, wide), 1) >> 6) == iota((heads, wide), 0)).astype(F32)


def head_rows(heads, wide):
    return ((iota((wide, heads), 0) >> 6) == iota((wide, heads), 1)).astype(F32)


def clocks(raw_t, rate):
    step = softplus(raw_t).T
    logs = -step * rate
    tok = logs.shape[0]
    upto = (iota((tok, tok), 0) >= iota((tok, tok), 1)).astype(F32)
    return step, exact(upto, logs)


def routing(ids_t, experts):
    numbers = iota((experts, ids_t.shape[1]), 0)
    first, second = ids_t[0:1, :] == numbers, ids_t[1:2, :] == numbers
    named = jnp.where(first, 1.0, jnp.where(second, 1.0, 0.0))
    tok = ids_t.shape[1]
    earlier = (iota((tok, tok), 0) < iota((tok, tok), 1)).astype(F32)
    before = mm(named, earlier)
    key = jnp.where(named > 0.0, before, -1.0)
    shape = (experts, SLOTS, tok)
    pick = jnp.broadcast_to(key[:, None, :], shape) == iota(shape, 1).astype(F32)
    return first, second, jnp.where(pick, 1.0, 0.0)


def put_tiles(out_ref, rows, experts):
    cols = rows.shape[1] // LANES
    tiled = rows.reshape(experts, SLOTS, rows.shape[1])
    for col in range(cols):
        out_ref[:, col * SLOTS : (col + 1) * SLOTS, :] = tiled[
            :, :, col * LANES : (col + 1) * LANES
        ].astype(BF16)


def put_pieces(out_ref, at, state):
    rows = state.shape[0] // 8
    for col in range(state.shape[1] // LANES):
        piece = state[:, col * LANES : (col + 1) * LANES].reshape(rows, 8, LANES)
        out_ref[col * rows : (col + 1) * rows, at : at + 8, :] = piece.astype(BF16)


def get_pieces(pieces):
    rows = STATE // 8
    cols = pieces.shape[0] // rows
    return jnp.concatenate(
        [pieces[col * rows : (col + 1) * rows].reshape(STATE, LANES) for col in range(cols)],
        axis=1,
    )


def enter_kernel(ids_ref, moe_ref, out_ref):
    experts = out_ref.shape[0]
    pick = routing(ids_ref[...], experts)[2]
    put_tiles(out_ref, mm(pick.reshape(experts * SLOTS, -1), moe_ref[...]), experts)


def put_fresh(x_ref, b_ref, raw_ref, rate_ref, out_ref):
    step, running = clocks(raw_ref[...], rate_ref[...])
    heads, wide = step.shape[1], x_ref.shape[1]
    last = running[-1:, :]
    spread = exact(
        jnp.concatenate(
            [step * jnp.exp(last - running), jnp.broadcast_to(jnp.exp(last), (8, heads))], axis=0
        ),
        head_lanes(heads, wide),
    )
    x = x_ref[...].astype(F32)
    at_end = x * sigmoid(x) * spread[:-8]
    b = b_ref[...].astype(F32)
    put_pieces(out_ref, 32, mm(b * sigmoid(b), at_end))
    total = spread[-8:]
    high = total.astype(BF16).astype(F32)
    mid = (total - high).astype(BF16).astype(F32)
    low = total - high - mid
    row = iota(total.shape, 0)
    tile = jnp.where(row == 0, high, jnp.where(row == 1, mid, jnp.where(row == 2, low, 0.0)))
    rows_at = STATE // 8
    for col in range(wide // LANES):
        part = tile[:, col * LANES : (col + 1) * LANES].astype(BF16)
        out_ref[col * rows_at : (col + 1) * rows_at, 40:48, :] = jnp.broadcast_to(
            part[None], (rows_at, 8, LANES)
        )


def weigh_kernel(ids_ref, weights_ref, cot_ref, x_ref, b_ref, raw_ref, rate_ref, out_ref):
    put_fresh(x_ref, b_ref, raw_ref, rate_ref, out_ref)
    experts = out_ref.shape[0]
    first, second, pick = routing(ids_ref[...], experts)
    weights = weights_ref[...]
    weight_at = jnp.where(first, weights[0:1, :], 0.0) + jnp.where(second, weights[1:2, :], 0.0)
    scaling = jnp.sum(
        pick * jnp.broadcast_to(weight_at[:, None, :], pick.shape), axis=2, keepdims=True
    )
    rows = mm(pick.reshape(experts * SLOTS, -1), cot_ref[...])
    put_tiles(
        out_ref,
        (rows.reshape(experts, SLOTS, -1) * scaling).reshape(experts * SLOTS, -1),
        experts,
    )


def block_decays(got_ref):
    tile = got_ref[:, 40:48, :].astype(F32)
    total = tile[:, 0:1, :] + tile[:, 1:2, :] + tile[:, 2:3, :]
    return jnp.broadcast_to(total, tile.shape)


def ahead_kernel(got_ref, out_ref):
    decays = block_decays(got_ref)
    pieces = got_ref[:, 32:40, :].astype(F32)
    total = jnp.zeros(pieces.shape[1:], F32)
    found = []
    for k in range(pieces.shape[0]):
        found.append(total)
        total = total * decays[k] + pieces[k]
    out_ref[...] = jnp.stack(found, axis=0).astype(BF16)


def behind_kernel(got_ref, pieces_ref, out_ref):
    decays = block_decays(got_ref)
    pieces = pieces_ref[...].astype(F32)
    total = jnp.zeros(pieces.shape[1:], F32)
    found = []
    for k in reversed(range(pieces.shape[0])):
        found.append(total)
        total = total * decays[k] + pieces[k]
    out_ref[...] = jnp.stack(found[::-1], axis=0).astype(BF16)


def first_kernel(here_ref, own_ref, left_ref, right_ref, far_ref, gate_ref, up_ref, out_gate_ref, out_up_ref):
    here = here_ref[0]
    for weight_ref, out_ref in ((gate_ref, out_gate_ref), (up_ref, out_up_ref)):
        total = None
        for block_ref, offset in ((own_ref, 0), (left_ref, 3), (right_ref, 1), (far_ref, 2)):
            width = block_ref.shape[1]
            at = pl.multiple_of(((here + offset) & 3) * width, width)
            term = mm(block_ref[...], weight_ref[pl.ds(at, width), :])
            total = term if total is None else total + term
        out_ref[...] = total


def middle_kernel(
    here_ref, own_ref, left_ref, right_ref, op_ref, down_ref, pre_ref, up_pre_ref, gate_ref, up_ref,
    hidden_ref, gate_grad_ref, up_grad_ref, far_ref, next_ref, back_ref, rest_ref,
):
    here = here_ref[0]
    hidden_grad = None
    for block_ref, offset in ((own_ref, 0), (left_ref, 3), (right_ref, 1), (op_ref, 2)):
        width = block_ref.shape[1]
        at = pl.multiple_of(((here + offset) & 3) * width, width)
        term = mm_nt(block_ref[...], down_ref[:, pl.ds(at, width)])
        hidden_grad = term if hidden_grad is None else hidden_grad + term
    pre, up_pre = pre_ref[...], up_pre_ref[...]
    sig = sigmoid(pre)
    active = pre * sig
    hidden_ref[...] = (active * up_pre).astype(BF16)
    gate_grad = (hidden_grad * up_pre * sig * (1.0 + pre * (1.0 - sig))).astype(BF16)
    up_grad = (hidden_grad * active).astype(BF16)
    gate_grad_ref[...] = gate_grad
    up_grad_ref[...] = up_grad
    width = rest_ref.shape[1]
    for offset, term_ref in ((2, far_ref), (1, next_ref), (3, back_ref), (0, rest_ref)):
        at = pl.multiple_of(((here + offset) & 3) * width, width)
        term = mm_nt(gate_grad, gate_ref[pl.ds(at, width), :]) + mm_nt(
            up_grad, up_ref[pl.ds(at, width), :]
        )
        term_ref[...] = term.astype(BF16)


def weights_kernel(
    here_ref, in0_ref, in1_ref, in2_ref, in3_ref, out0_ref, out1_ref, out2_ref, out3_ref,
    hidden_ref, gate_grad_ref, up_grad_ref, gate_ref, up_ref, down_ref,
):
    here = here_ref[0]
    hidden_t = hidden_ref[...].T
    for in_ref, grad_ref, offset in (
        (in0_ref, out0_ref, 0), (in1_ref, out1_ref, 3), (in2_ref, out2_ref, 1), (in3_ref, out3_ref, 2)
    ):
        width = in_ref.shape[1]
        at = pl.multiple_of(((here + offset) & 3) * width, width)
        block_t = in_ref[...].T
        gate_ref[pl.ds(at, width), :] = mm(block_t, gate_grad_ref[...]).astype(BF16)
        up_ref[pl.ds(at, width), :] = mm(block_t, up_grad_ref[...]).astype(BF16)
        down_ref[:, pl.ds(at, width)] = mm(hidden_t, grad_ref[...]).astype(BF16)


def combine_kernel(ids_ref, cot_ref, back_ref, out_ref):
    experts = back_ref.shape[0] // SLOTS
    pick = routing(ids_ref[...], experts)[2].reshape(experts * SLOTS, -1)
    moe_grad = mm(pick.T, back_ref[...])
    rows = (cot_ref[...].astype(F32) + moe_grad).astype(BF16)
    for k in range(out_ref.shape[0]):
        out_ref[k] = rows


def halves(value):
    low = iota(value.shape, 1) < HEAD_DIM
    return jnp.where(low, value, 0.0), jnp.where(low, 0.0, value)


def fade_of(column, row, keep):
    return jnp.exp(jnp.where(keep, column - row, -1e30))


def forward_kernel(
    x_ref, z_ref, b_ref, c_ref, raw_ref, rate_ref, skip_ref, gain_ref, got_ref,
    norm_ref, mixed_ref, start_ref, wide_ref,
):
    start = get_pieces(got_ref[...].astype(F32))
    start_ref[...] = start.astype(BF16)
    step, running = clocks(raw_ref[...], rate_ref[...])
    tok, heads = step.shape
    wide = x_ref.shape[1]
    spread = exact(
        jnp.concatenate(
            [step, jnp.exp(running), jnp.broadcast_to(skip_ref[...], (8, heads))], axis=0
        ),
        head_lanes(heads, wide),
    )
    x = x_ref[...].astype(F32)
    x_act = x * sigmoid(x)
    scaled = x_act * spread[:tok]
    wide_ref[...] = spread[tok : 2 * tok]
    b, c = b_ref[...].astype(F32), c_ref[...].astype(F32)
    b_t, c_t = b * sigmoid(b), c * sigmoid(c)
    c_act = c_t.T
    scores = mm(c_act, b_t)
    mixed = spread[tok : 2 * tok] * mm(c_act, start) + x_act * spread[2 * tok : 2 * tok + 1]
    running_t = running.T
    keep = iota((tok, tok), 0) >= iota((tok, tok), 1)
    for pair in range(heads // 2):
        lanes = slice(pair * LANES, (pair + 1) * LANES)
        mixes = [
            scores * fade_of(running[:, h : h + 1], running_t[h : h + 1, :], keep)
            for h in (2 * pair, 2 * pair + 1)
        ]
        inside = mm(
            jnp.concatenate(mixes, axis=1), jnp.concatenate(halves(scaled[:, lanes]), axis=0)
        )
        mixed_ref[:, lanes] = mixed[:, lanes] + inside
    z = z_ref[...].astype(F32)
    gated = mixed_ref[...] * (z * sigmoid(z))
    scale = lax.rsqrt(jnp.mean(gated * gated, axis=1, keepdims=True) + EPS)
    norm_ref[...] = (gated * scale * gain_ref[...]).astype(BF16)


def gate_back_kernel(
    rows_ref, w_ref, mixed_ref, z_ref, gain_ref, wide_ref, c_ref, pieces_ref, grad_z_ref, d_mixed_ref
):
    z = z_ref[...].astype(F32)
    sig = sigmoid(z)
    z_act = z * sig
    mixed = mixed_ref[...]
    gated = mixed * z_act
    scale = lax.rsqrt(jnp.mean(gated * gated, axis=1, keepdims=True) + EPS)
    rows = jnp.concatenate([rows_ref[k] for k in range(rows_ref.shape[0])], axis=1)
    d_norm = mm(rows, w_ref[...]) * gain_ref[...]
    along_row = jnp.mean(d_norm * gated, axis=1, keepdims=True)
    d_gated = scale * d_norm - gated * (scale * scale * scale * along_row)
    d_mixed = d_gated * z_act
    c = c_ref[...].astype(F32)
    put_pieces(pieces_ref, 0, mm(c * sigmoid(c), d_mixed * wide_ref[...]))
    d_mixed_ref[...] = d_mixed
    grad_z_ref[...] = (d_gated * mixed * (sig * (1.0 + z * (1.0 - sig)))).astype(BF16)


def project_kernel(*refs):
    plane, row = refs[0][0], refs[0][1]
    part_refs, near_ref, far_ref = refs[1:5], refs[5], refs[6]
    own_ref, share_refs, left_ref = refs[7], refs[8:15], refs[15]
    tok = near_ref.shape[1]
    planes, rows = part_refs[0].shape[1], part_refs[0].shape[2]
    for step in range(planes):
        for k, part_ref in enumerate(part_refs):
            for half in (0, 1):
                at = (2 * k + half) * tok
                left_ref[step * rows : (step + 1) * rows, at : at + tok] = part_ref[
                    half, (plane + step) & (planes - 1)
                ]
    total = None
    for k in range(4):
        for half, block_ref in enumerate((near_ref, far_ref)):
            at = (2 * k + half) * tok
            term = mm(left_ref[:, at : at + tok], block_ref[(row - k) & 3])
            total = term if total is None else total + term
    own_ref[...] = total[:rows]
    for step in range(1, planes):
        share_refs[step - 1][...] = total[step * rows : (step + 1) * rows].astype(BF16)


def inside_back_kernel(
    x_ref, b_ref, c_ref, raw_ref, rate_ref, skip_ref, start_ref, wide_ref, d_mixed_ref,
    grad_x_ref, reach_x_ref, reach_s_ref, at_end_ref, d_b_ref, grad_c_ref, small_ref,
    d_scaled_ref,
):
    step, running = clocks(raw_ref[...], rate_ref[...])
    tok, heads = step.shape
    wide = x_ref.shape[1]
    last = running[-1:, :]
    spread = exact(
        jnp.concatenate(
            [step, jnp.exp(last - running), jnp.broadcast_to(skip_ref[...], (8, heads))], axis=0
        ),
        head_lanes(heads, wide),
    )
    step_wide, end_wide = spread[:tok], spread[tok : 2 * tok]
    x = x_ref[...].astype(F32)
    sig = sigmoid(x)
    x_act = x * sig
    scaled = x_act * step_wide
    d_mixed = d_mixed_ref[...]
    b, c = b_ref[...].astype(F32), c_ref[...].astype(F32)
    sig_c = sigmoid(c)
    b_t, c_t = b * sigmoid(b), c * sig_c
    b_act, c_act = b_t.T, c_t.T
    scores, scores_t = mm(c_act, b_t), mm(b_act, c_t)
    running_t = running.T
    rows, cols = iota((tok, tok), 0), iota((tok, tok), 1)
    keep, keep_t = rows >= cols, rows <= cols
    d_scores = jnp.zeros((tok, tok), F32)
    gained = jnp.zeros((tok, heads), F32)
    lost = jnp.zeros((heads, tok), F32)
    head_at, head_row = iota((tok, heads), 1), iota((heads, tok), 0)
    for pair in range(heads // 2):
        lanes = slice(pair * LANES, (pair + 1) * LANES)
        d_parts = halves(d_mixed[:, lanes])
        mixes_t = []
        for half in (0, 1):
            h = 2 * pair + half
            column, row = running[:, h : h + 1], running_t[h : h + 1, :]
            fade = fade_of(column, row, keep)
            mixes_t.append(scores_t * jnp.exp(jnp.where(keep_t, row - column, -1e30)))
            d_fade = mm_nt(d_parts[half], scaled[:, lanes]) * fade
            d_scores = d_scores + d_fade
            flow = d_fade * scores
            gained = jnp.where(head_at == h, jnp.sum(flow, axis=1, keepdims=True), gained)
            lost = jnp.where(head_row == h, jnp.sum(flow, axis=0, keepdims=True), lost)
        d_scaled_ref[:, lanes] = mm(
            jnp.concatenate(mixes_t, axis=1), jnp.concatenate(d_parts, axis=0)
        )
    start = start_ref[...].astype(F32)
    d_carried = d_mixed * wide_ref[...]
    by_head = head_rows(heads, wide)
    d_scaled = d_scaled_ref[...]
    d_run = gained - lost.T + exact(d_carried * mm(c_act, start), by_head)
    d_step = exact(d_scaled * x_act, by_head)
    small_ref[0] = d_run
    small_ref[1] = d_step
    small_ref[2] = jnp.broadcast_to(jnp.exp(last), (tok, heads))
    d_silu = sig * (1.0 + x * (1.0 - sig))
    grad_x_ref[...] = (d_scaled * step_wide + d_mixed * spread[2 * tok : 2 * tok + 1]) * d_silu
    reach_x_ref[...] = end_wide * step_wide * d_silu
    reach_s_ref[...] = end_wide * x_act
    at_end_ref[...] = (scaled * end_wide).astype(BF16)
    d_b_ref[...] = mm(c_t, d_scores)
    d_c = mm_nt(b_t, d_scores) + mm_nt(start, d_carried)
    grad_c_ref[...] = d_c * (sig_c * (1.0 + c * (1.0 - sig_c)))


def leave_kernel(
    pieces_ref, start_ref, b_ref, raw_ref, rate_ref, base_ref, reach_x_ref, reach_s_ref,
    at_end_ref, d_b_ref, small_ref, grad_x_ref, grad_b_ref, grad_step_ref,
):
    after = get_pieces(pieces_ref[...].astype(F32))
    b = b_ref[...].astype(F32)
    sig_b = sigmoid(b)
    reach = mm((b * sig_b).T, after)
    grad_x_ref[...] = (base_ref[...] + reach * reach_x_ref[...]).astype(BF16)
    tok, wide = reach.shape
    raw = raw_ref[...]
    step = softplus(raw).T
    heads = step.shape[1]
    both = jnp.concatenate(
        [
            reach * reach_s_ref[...],
            jnp.broadcast_to(
                jnp.sum(after * start_ref[...].astype(F32), axis=0, keepdims=True), (8, wide)
            ),
        ],
        axis=0,
    )
    sums = exact(both, head_rows(heads, wide))
    lost = step * sums[:tok]
    d_run = small_ref[0] - lost
    end_part = jnp.sum(lost, axis=0, keepdims=True) + small_ref[2][:1] * sums[tok : tok + 1]
    onward = (iota((tok, tok), 0) <= iota((tok, tok), 1)).astype(F32)
    d_log = exact(onward, d_run) + end_part
    d_step = small_ref[1] + sums[:tok] - d_log * rate_ref[...]
    grad_step_ref[...] = d_step.T * sigmoid(raw)
    d_b = d_b_ref[...] + mm_nt(after, at_end_ref[...])
    grad_b_ref[...] = d_b * (sig_b * (1.0 + b * (1.0 - sig_b)))


class Held:
    def __init__(self, array):
        self.array = array


def local(kernel, outs, args, flops, scratch=(), scalars=0, away=()):
    outs = outs if isinstance(outs, tuple) else (outs,)
    outs = tuple(pltpu.HBM(o.shape, o.dtype) if i in away else o for i, o in enumerate(outs))
    held = [i for i, a in enumerate(args) if isinstance(a, Held)]
    arrays = [
        pltpu.with_memory_space_constraint(a.array, pltpu.HBM) if isinstance(a, Held) else a
        for a in args
    ]
    spaces = [
        pltpu.SMEM if i < scalars else pltpu.HBM if i in held else pltpu.VMEM
        for i in range(len(args))
    ]
    count = len(args) + len(outs) + len(scratch)

    def run(*refs):
        refs, inside, sems = list(refs[:count]), refs[count:-1], refs[-1]
        copies = []
        for k, i in enumerate(held):
            copies.append(pltpu.make_async_copy(refs[i], inside[k], sems.at[k]))
            copies[-1].start()
            refs[i] = inside[k]
        for copy in copies:
            copy.wait()
        kernel(*refs)

    call = pl.pallas_call(
        run if held else kernel,
        out_shape=outs,
        scratch_shapes=(
            *scratch,
            *[pltpu.VMEM(arrays[i].shape, arrays[i].dtype) for i in held],
            *([pltpu.SemaphoreType.DMA((len(held),))] if held else []),
        ),
        in_specs=[pl.BlockSpec(memory_space=space) for space in spaces],
        compiler_params=pltpu.CompilerParams(vmem_limit_bytes=16 << 20),
        cost_estimate=pl.CostEstimate(flops=flops, bytes_accessed=1 << 21, transcendentals=1 << 18),
    )
    found = call(*arrays)
    return found if len(outs) > 1 else found[0]


def body(
    moe_input,
    cotangent,
    expert_ids,
    routing_weights,
    gate_weight,
    up_weight,
    down_weight,
    inner_x,
    inner_b,
    inner_c,
    gate_z,
    step_raw,
    decay_rate,
    skip_weight,
    norm_gain,
    w_out,
):
    tok = expert_ids.shape[0]
    heads = decay_rate.shape[0]
    experts = lax.axis_size(SP)
    wide = inner_x.shape[1]
    gate_w, up_w, down_w = gate_weight[0], up_weight[0], down_weight[0]
    ids_t, b_t, c_t, raw_t = expert_ids.T, inner_b.T, inner_c.T, step_raw.T
    rate, skip, gain = decay_rate[None, :], skip_weight[None, :], norm_gain[None, :]
    here = lax.axis_index("x")[None]
    shape = jax.ShapeDtypeStruct
    slots = experts * SLOTS
    cols, inner = moe_input.shape[1], gate_w.shape[1]

    sent_in = local(
        enter_kernel, shape((experts, 32, LANES), BF16), (Held(ids_t), Held(moe_input)), SMALL
    )
    got_in = to_all(sent_in, SP)
    sent_grad = local(
        weigh_kernel,
        shape((experts, 48, LANES), BF16),
        (Held(ids_t), Held(routing_weights.T), Held(cotangent), Held(inner_x), Held(b_t), Held(raw_t), Held(rate)),
        SMALL,
    )
    got_grad = to_all(sent_grad, SP)

    rows_in = rows_of(got_in)
    in_left, in_right, in_far = around(rows_in)
    pre, up_pre = local(
        first_kernel,
        (shape((slots, inner), F32), shape((slots, inner), F32)),
        (here, rows_in, in_left, in_right, in_far, Held(gate_w), Held(up_w)),
        SMALL,
        scalars=1,
        away=(0, 1),
    )
    rows_grad = rows_of(got_grad[:, :32])
    grad_left, grad_right, grad_far = around(rows_grad)

    pieces = local(ahead_kernel, shape((experts, 8, LANES), BF16), (got_grad,), SMALL)
    pieces = to_all(pieces, SP)

    hidden, gate_grad, up_grad, term_far, term_next, term_back, term_own = local(
        middle_kernel,
        (
            shape((slots, inner), BF16),
            shape((slots, inner), BF16),
            shape((slots, inner), BF16),
            *[shape((slots, cols), BF16)] * 4,
        ),
        (here, rows_grad, grad_left, grad_right, grad_far, Held(down_w), Held(pre), Held(up_pre), Held(gate_w), Held(up_w)),
        SMALL,
        scalars=1,
        away=(0, 1, 2),
    )
    terms = shifted(term_far, 2), shifted(term_next, 1), shifted(term_back, -1)
    slot_grad = term_own.astype(F32)
    for term in terms:
        slot_grad = slot_grad + term.astype(F32)
    slot_grad = slot_grad.astype(BF16)

    norm_rows, mixed, start_state, start_wide = local(
        forward_kernel,
        (
            shape((tok, wide), BF16),
            shape((tok, wide), F32),
            shape((STATE, wide), BF16),
            shape((tok, wide), F32),
        ),
        (Held(inner_x), Held(gate_z), Held(b_t), Held(c_t), Held(raw_t), Held(rate), Held(skip), Held(gain), pieces),
        SMALL,
        away=(1, 2, 3),
    )
    norm_y = to_all(jnp.broadcast_to(norm_rows[None], (4, tok, wide)), "y")
    slot_grad, norm_y = lax.optimization_barrier((slot_grad, norm_y))
    back = to_all(slot_grad.reshape(experts, SLOTS, -1), SP).reshape(slots, -1)
    norm_c = along(norm_y, "c", 1)
    gate_out, up_out, down_out = local(
        weights_kernel,
        (
            shape(gate_w.shape, BF16),
            shape(up_w.shape, BF16),
            shape(down_w.shape, BF16),
        ),
        (
            here,
            *[
                Held(a)
                for a in (
                    rows_in, in_left, in_right, in_far, rows_grad, grad_left, grad_right, grad_far,
                    hidden, gate_grad, up_grad,
                )
            ],
        ),
        LARGE,
        scalars=1,
    )

    mixer_cols = local(
        combine_kernel,
        shape((4, *cotangent.shape), BF16),
        (Held(ids_t), Held(cotangent), back),
        SMALL,
    )
    mixer4 = to_all(mixer_cols, "x")

    pieces, grad_z, d_mixed = local(
        gate_back_kernel,
        (
            shape((experts, 8, LANES), BF16),
            shape((tok, wide), BF16),
            shape((tok, wide), F32),
        ),
        (mixer4, Held(w_out), Held(mixed), Held(gate_z), Held(gain), Held(start_wide), Held(c_t)),
        SMALL,
        away=(2,),
    )

    mine, row, plane = lax.axis_index("c"), lax.axis_index("y"), lax.axis_index("z")
    mixer_t = mixer4.transpose(0, 2, 1).reshape(8, 4, 2, 32, tok).transpose(2, 1, 0, 3, 4)
    pieces = to_all(pieces, SP)
    keep = lax.dynamic_index_in_dim(mixer_t, mine, 0, keepdims=False)
    give = lax.dynamic_index_in_dim(mixer_t, 1 - mine, 0, keepdims=False)
    take = along(give, "c", 1)
    both = jnp.stack([keep, take], axis=0)
    parts = [lax.dynamic_index_in_dim(both, row, 1, keepdims=False)] + [
        along(lax.dynamic_index_in_dim(both, (row + step) % 4, 1, keepdims=False), "y", step)
        for step in (1, 2, 3)
    ]
    found = local(
        project_kernel,
        (shape((32, wide), F32), *[shape((32, wide), BF16)] * 7),
        (jnp.stack([plane, row]), *parts, norm_y, norm_c),
        SMALL,
        (pltpu.VMEM((256, 8 * tok), BF16),),
        scalars=1,
    )
    grad_out = found[0]
    for step in (4, 3, 5, 2, 6, 1, 7):
        share = along(found[step], "z", step)
        grad_out = grad_out + share.astype(F32)
    pieces = local(behind_kernel, shape((experts, 8, LANES), BF16), (got_grad, pieces), SMALL)
    pieces = to_all(pieces, SP)
    grad_x, reach_x, reach_s, at_end, d_b, grad_c, small = local(
        inside_back_kernel,
        (
            shape((tok, wide), F32),
            shape((tok, wide), F32),
            shape((tok, wide), F32),
            shape((tok, wide), BF16),
            shape((STATE, tok), F32),
            shape((STATE, tok), F32),
            shape((3, tok, heads), F32),
        ),
        (Held(inner_x), Held(b_t), Held(c_t), Held(raw_t), Held(rate), Held(skip), Held(start_state), Held(start_wide), Held(d_mixed)),
        LARGE,
        (pltpu.VMEM((tok, wide), F32),),
        away=tuple(range(7)),
    )
    grad_x, grad_b, grad_step = local(
        leave_kernel,
        (shape((tok, wide), BF16), shape((STATE, tok), F32), shape((heads, tok), F32)),
        (
            pieces,
            *[
                Held(a)
                for a in (start_state, b_t, raw_t, rate, grad_x, reach_x, reach_s, at_end, d_b, small)
            ],
        ),
        SMALL,
    )
    return (
        gate_out[None],
        up_out[None],
        down_out[None],
        grad_out,
        grad_x,
        grad_b.T,
        grad_c.T,
        grad_z,
        grad_step.T,
    )


def solution(mesh):
    finer = Mesh(mesh.devices.reshape(8, 4, 2, mesh.shape["tp"]), ("z", "y", "c", "x"))
    return jax.shard_map(
        body,
        mesh=finer,
        in_specs=(
            P(SP, "x"),
            P(SP, "x"),
            P(SP, None),
            P(SP, None),
            P(SP, None, "x"),
            P(SP, None, "x"),
            P(SP, "x", None),
            P(SP, "x"),
            P(SP, "x"),
            P(SP, "x"),
            P(SP, "x"),
            P(SP, "x"),
            P("x"),
            P("x"),
            P("x"),
            P(None, "x"),
        ),
        out_specs=(
            P(SP, None, "x"),
            P(SP, None, "x"),
            P(SP, "x", None),
            P(SP, "x"),
            P(SP, "x"),
            P(SP, "x"),
            P(SP, "x"),
            P(SP, "x"),
            P(SP, "x"),
        ),
        check_vma=False,
    )
```

```python
import jax
import jax.numpy as jnp
from jax import lax
from jax.sharding import Mesh
from jax.experimental import pallas as pl
from jax.experimental.pallas import tpu as pltpu
from jax.sharding import PartitionSpec as P

HEAD_DIM = 64
STATE = 64
LANES = 128
SLOTS = 8
EPS = 0.01
SP = ("z", "y", "c")
F32 = jnp.float32
BF16 = jnp.bfloat16
HIGH = lax.Precision.HIGHEST


def along(value, axis, step):
    count = lax.axis_size(axis)
    return lax.ppermute(value, axis, [(i, (i + step) % count) for i in range(count)])


def shifted(value, step):
    return along(value, "x", step)


def to_all(value, axes):
    return lax.all_to_all(value, axes, split_axis=0, concat_axis=0, tiled=True)


def around(value):
    return shifted(value, 1), shifted(value, -1), shifted(value, 2)


def rows_of(tiled):
    cols = tiled.shape[1] // SLOTS
    rows = tiled.reshape(-1, cols, SLOTS, LANES).transpose(0, 2, 1, 3)
    return rows.reshape(-1, cols * LANES)


SMALL, LARGE = 1 << 30, 1 << 32


def staged_kernel(*refs):
    half = len(refs) // 2
    copies = [
        pltpu.make_async_copy(source, target, refs[-1].at[k])
        for k, (source, target) in enumerate(zip(refs[:half], refs[half:-1]))
    ]
    for copy in copies:
        copy.start()
    for copy in copies:
        copy.wait()


def staged(arrays):
    return pl.pallas_call(
        staged_kernel,
        out_shape=tuple(pltpu.VMEM(a.shape, a.dtype) for a in arrays),
        in_specs=[pl.BlockSpec(memory_space=pltpu.HBM)] * len(arrays),
        scratch_shapes=(pltpu.SemaphoreType.DMA((len(arrays),)),),
        compiler_params=pltpu.CompilerParams(vmem_limit_bytes=16 << 20),
        cost_estimate=pl.CostEstimate(flops=SMALL, bytes_accessed=1 << 22, transcendentals=0),
    )(*[pltpu.with_memory_space_constraint(a, pltpu.HBM) for a in arrays])


def softplus(value):
    small = jnp.exp(-jnp.abs(value))
    grown = 1.0 + small
    log_part = jnp.where(
        grown == 1.0, small, jnp.log(grown) * (small / jnp.where(grown == 1.0, 1.0, grown - 1.0))
    )
    return jnp.maximum(value, 0.0) + log_part


def sigmoid(value):
    return 1.0 / (1.0 + jnp.exp(-value))


def mm(left, right):
    return jnp.dot(left.astype(BF16), right.astype(BF16), preferred_element_type=F32)


def mm_nt(left, right):
    return lax.dot_general(
        left.astype(BF16),
        right.astype(BF16),
        (((1,), (1,)), ((), ())),
        preferred_element_type=F32,
    )


def exact(left, right):
    return jnp.dot(left, right, preferred_element_type=F32, precision=HIGH)


def iota(shape, dim):
    return lax.broadcasted_iota(jnp.int32, shape, dim)


def head_lanes(heads, wide):
    return ((iota((heads, wide), 1) >> 6) == iota((heads, wide), 0)).astype(F32)


def head_rows(heads, wide):
    return ((iota((wide, heads), 0) >> 6) == iota((wide, heads), 1)).astype(F32)


def clocks(raw_t, rate):
    step = softplus(raw_t).T
    logs = -step * rate
    tok = logs.shape[0]
    upto = (iota((tok, tok), 0) >= iota((tok, tok), 1)).astype(F32)
    return step, exact(upto, logs)


def routing(ids_t, experts):
    numbers = iota((experts, ids_t.shape[1]), 0)
    first, second = ids_t[0:1, :] == numbers, ids_t[1:2, :] == numbers
    named = jnp.where(first, 1.0, jnp.where(second, 1.0, 0.0))
    tok = ids_t.shape[1]
    earlier = (iota((tok, tok), 0) < iota((tok, tok), 1)).astype(F32)
    before = mm(named, earlier)
    key = jnp.where(named > 0.0, before, -1.0)
    shape = (experts, SLOTS, tok)
    pick = jnp.broadcast_to(key[:, None, :], shape) == iota(shape, 1).astype(F32)
    return first, second, jnp.where(pick, 1.0, 0.0)


def put_tiles(out_ref, rows, experts):
    cols = rows.shape[1] // LANES
    tiled = rows.reshape(experts, SLOTS, rows.shape[1])
    for col in range(cols):
        out_ref[:, col * SLOTS : (col + 1) * SLOTS, :] = tiled[
            :, :, col * LANES : (col + 1) * LANES
        ].astype(BF16)


def put_pieces(out_ref, at, state):
    rows = state.shape[0] // 8
    for col in range(state.shape[1] // LANES):
        piece = state[:, col * LANES : (col + 1) * LANES].reshape(rows, 8, LANES)
        out_ref[col * rows : (col + 1) * rows, at : at + 8, :] = piece.astype(BF16)


def get_pieces(pieces):
    rows = STATE // 8
    cols = pieces.shape[0] // rows
    return jnp.concatenate(
        [pieces[col * rows : (col + 1) * rows].reshape(STATE, LANES) for col in range(cols)],
        axis=1,
    )


def enter_kernel(ids_ref, moe_ref, out_ref):
    experts = out_ref.shape[0]
    pick = routing(ids_ref[...], experts)[2]
    put_tiles(out_ref, mm(pick.reshape(experts * SLOTS, -1), moe_ref[...]), experts)


def put_fresh(x_ref, b_ref, raw_ref, rate_ref, out_ref):
    step, running = clocks(raw_ref[...], rate_ref[...])
    heads, wide = step.shape[1], x_ref.shape[1]
    last = running[-1:, :]
    spread = exact(
        jnp.concatenate(
            [step * jnp.exp(last - running), jnp.broadcast_to(jnp.exp(last), (8, heads))], axis=0
        ),
        head_lanes(heads, wide),
    )
    x = x_ref[...].astype(F32)
    at_end = x * sigmoid(x) * spread[:-8]
    b = b_ref[...].astype(F32)
    put_pieces(out_ref, 32, mm(b * sigmoid(b), at_end))
    total = spread[-8:]
    high = total.astype(BF16).astype(F32)
    mid = (total - high).astype(BF16).astype(F32)
    low = total - high - mid
    row = iota(total.shape, 0)
    tile = jnp.where(row == 0, high, jnp.where(row == 1, mid, jnp.where(row == 2, low, 0.0)))
    rows_at = STATE // 8
    for col in range(wide // LANES):
        part = tile[:, col * LANES : (col + 1) * LANES].astype(BF16)
        out_ref[col * rows_at : (col + 1) * rows_at, 40:48, :] = jnp.broadcast_to(
            part[None], (rows_at, 8, LANES)
        )


def weigh_kernel(ids_ref, weights_ref, cot_ref, x_ref, b_ref, raw_ref, rate_ref, out_ref):
    put_fresh(x_ref, b_ref, raw_ref, rate_ref, out_ref)
    experts = out_ref.shape[0]
    first, second, pick = routing(ids_ref[...], experts)
    weights = weights_ref[...]
    weight_at = jnp.where(first, weights[0:1, :], 0.0) + jnp.where(second, weights[1:2, :], 0.0)
    scaling = jnp.sum(
        pick * jnp.broadcast_to(weight_at[:, None, :], pick.shape), axis=2, keepdims=True
    )
    rows = mm(pick.reshape(experts * SLOTS, -1), cot_ref[...])
    put_tiles(
        out_ref,
        (rows.reshape(experts, SLOTS, -1) * scaling).reshape(experts * SLOTS, -1),
        experts,
    )


def block_decays(got_ref):
    tile = got_ref[:, 40:48, :].astype(F32)
    total = tile[:, 0:1, :] + tile[:, 1:2, :] + tile[:, 2:3, :]
    return jnp.broadcast_to(total, tile.shape)


def ahead_kernel(got_ref, out_ref):
    decays = block_decays(got_ref)
    pieces = got_ref[:, 32:40, :].astype(F32)
    total = jnp.zeros(pieces.shape[1:], F32)
    found = []
    for k in range(pieces.shape[0]):
        found.append(total)
        total = total * decays[k] + pieces[k]
    out_ref[...] = jnp.stack(found, axis=0).astype(BF16)


def behind_kernel(got_ref, pieces_ref, out_ref):
    decays = block_decays(got_ref)
    pieces = pieces_ref[...].astype(F32)
    total = jnp.zeros(pieces.shape[1:], F32)
    found = []
    for k in reversed(range(pieces.shape[0])):
        found.append(total)
        total = total * decays[k] + pieces[k]
    out_ref[...] = jnp.stack(found[::-1], axis=0).astype(BF16)


def first_kernel(here_ref, own_ref, left_ref, right_ref, far_ref, gate_ref, up_ref, out_gate_ref, out_up_ref):
    here = here_ref[0]
    for weight_ref, out_ref in ((gate_ref, out_gate_ref), (up_ref, out_up_ref)):
        total = None
        for block_ref, offset in ((own_ref, 0), (left_ref, 3), (right_ref, 1), (far_ref, 2)):
            width = block_ref.shape[1]
            at = pl.multiple_of(((here + offset) & 3) * width, width)
            term = mm(block_ref[...], weight_ref[pl.ds(at, width), :])
            total = term if total is None else total + term
        out_ref[...] = total


def hidden_kernel(
    here_ref, own_ref, left_ref, right_ref, op_ref, down_ref, pre_ref, up_pre_ref, gate_ref, up_ref,
    hidden_ref, gate_grad_ref, up_grad_ref, term_ref,
):
    here = here_ref[0]
    hidden_grad = None
    for block_ref, offset in ((own_ref, 0), (left_ref, 3), (right_ref, 1), (op_ref, 2)):
        width = block_ref.shape[1]
        at = pl.multiple_of(((here + offset) & 3) * width, width)
        term = mm_nt(block_ref[...], down_ref[:, pl.ds(at, width)])
        hidden_grad = term if hidden_grad is None else hidden_grad + term
    pre, up_pre = pre_ref[...], up_pre_ref[...]
    sig = sigmoid(pre)
    active = pre * sig
    hidden_ref[...] = (active * up_pre).astype(BF16)
    gate_grad = (hidden_grad * up_pre * sig * (1.0 + pre * (1.0 - sig))).astype(BF16)
    up_grad = (hidden_grad * active).astype(BF16)
    gate_grad_ref[...] = gate_grad
    up_grad_ref[...] = up_grad
    width = term_ref.shape[1]
    at = pl.multiple_of(((here + 2) & 3) * width, width)
    term_ref[...] = (
        mm_nt(gate_grad, gate_ref[pl.ds(at, width), :]) + mm_nt(up_grad, up_ref[pl.ds(at, width), :])
    ).astype(BF16)


def terms_kernel(
    here_ref, gate_grad_ref, up_grad_ref, gate_ref, up_ref, next_ref, back_ref, rest_ref
):
    here = here_ref[0]
    gate_grad, up_grad = gate_grad_ref[...], up_grad_ref[...]
    width = rest_ref.shape[1]
    for offset, term_ref in ((1, next_ref), (3, back_ref), (0, rest_ref)):
        at = pl.multiple_of(((here + offset) & 3) * width, width)
        term = mm_nt(gate_grad, gate_ref[pl.ds(at, width), :]) + mm_nt(
            up_grad, up_ref[pl.ds(at, width), :]
        )
        term_ref[...] = term.astype(BF16)


def sum_kernel(own_ref, left_ref, right_ref, far_ref, out_ref):
    total = own_ref[...].astype(F32) + left_ref[...].astype(F32)
    total = total + right_ref[...].astype(F32) + far_ref[...].astype(F32)
    out_ref[...] = total.astype(BF16)


def weights_kernel(
    here_ref, in0_ref, in1_ref, in2_ref, in3_ref, out0_ref, out1_ref, out2_ref, out3_ref,
    hidden_ref, gate_grad_ref, up_grad_ref, gate_ref, up_ref, down_ref,
):
    here = here_ref[0]
    hidden_t = hidden_ref[...].T
    for in_ref, grad_ref, offset in (
        (in0_ref, out0_ref, 0), (in1_ref, out1_ref, 3), (in2_ref, out2_ref, 1), (in3_ref, out3_ref, 2)
    ):
        width = in_ref.shape[1]
        at = pl.multiple_of(((here + offset) & 3) * width, width)
        block_t = in_ref[...].T
        gate_ref[pl.ds(at, width), :] = mm(block_t, gate_grad_ref[...]).astype(BF16)
        up_ref[pl.ds(at, width), :] = mm(block_t, up_grad_ref[...]).astype(BF16)
        down_ref[:, pl.ds(at, width)] = mm(hidden_t, grad_ref[...]).astype(BF16)


def combine_kernel(ids_ref, cot_ref, back_ref, out_ref):
    experts = back_ref.shape[0] // SLOTS
    pick = routing(ids_ref[...], experts)[2].reshape(experts * SLOTS, -1)
    moe_grad = mm(pick.T, back_ref[...])
    rows = (cot_ref[...].astype(F32) + moe_grad).astype(BF16)
    for k in range(out_ref.shape[0]):
        out_ref[k] = rows


def halves(value):
    low = iota(value.shape, 1) < HEAD_DIM
    return jnp.where(low, value, 0.0), jnp.where(low, 0.0, value)


def fade_of(column, row, keep):
    return jnp.exp(jnp.where(keep, column - row, -1e30))


def forward_kernel(
    x_ref, z_ref, b_ref, c_ref, raw_ref, rate_ref, skip_ref, gain_ref, got_ref,
    norm_ref, mixed_ref, start_ref, wide_ref,
):
    start = get_pieces(got_ref[...].astype(F32))
    start_ref[...] = start.astype(BF16)
    step, running = clocks(raw_ref[...], rate_ref[...])
    tok, heads = step.shape
    wide = x_ref.shape[1]
    spread = exact(
        jnp.concatenate(
            [step, jnp.exp(running), jnp.broadcast_to(skip_ref[...], (8, heads))], axis=0
        ),
        head_lanes(heads, wide),
    )
    x = x_ref[...].astype(F32)
    x_act = x * sigmoid(x)
    scaled = x_act * spread[:tok]
    wide_ref[...] = spread[tok : 2 * tok]
    b, c = b_ref[...].astype(F32), c_ref[...].astype(F32)
    b_t, c_t = b * sigmoid(b), c * sigmoid(c)
    c_act = c_t.T
    scores = mm(c_act, b_t)
    mixed = spread[tok : 2 * tok] * mm(c_act, start) + x_act * spread[2 * tok : 2 * tok + 1]
    running_t = running.T
    keep = iota((tok, tok), 0) >= iota((tok, tok), 1)
    for pair in range(heads // 2):
        lanes = slice(pair * LANES, (pair + 1) * LANES)
        mixes = [
            scores * fade_of(running[:, h : h + 1], running_t[h : h + 1, :], keep)
            for h in (2 * pair, 2 * pair + 1)
        ]
        inside = mm(
            jnp.concatenate(mixes, axis=1), jnp.concatenate(halves(scaled[:, lanes]), axis=0)
        )
        mixed_ref[:, lanes] = mixed[:, lanes] + inside
    z = z_ref[...].astype(F32)
    gated = mixed_ref[...] * (z * sigmoid(z))
    scale = lax.rsqrt(jnp.mean(gated * gated, axis=1, keepdims=True) + EPS)
    norm_ref[...] = (gated * scale * gain_ref[...]).astype(BF16)


def gate_back_kernel(
    rows_ref, w_ref, mixed_ref, z_ref, gain_ref, wide_ref, c_ref, pieces_ref, grad_z_ref, d_mixed_ref
):
    z = z_ref[...].astype(F32)
    sig = sigmoid(z)
    z_act = z * sig
    mixed = mixed_ref[...]
    gated = mixed * z_act
    scale = lax.rsqrt(jnp.mean(gated * gated, axis=1, keepdims=True) + EPS)
    rows = jnp.concatenate([rows_ref[k] for k in range(rows_ref.shape[0])], axis=1)
    w_ref, arrived = w_ref
    arrived.wait()
    d_norm = mm(rows, w_ref[...]) * gain_ref[...]
    along_row = jnp.mean(d_norm * gated, axis=1, keepdims=True)
    d_gated = scale * d_norm - gated * (scale * scale * scale * along_row)
    d_mixed = d_gated * z_act
    c = c_ref[...].astype(F32)
    put_pieces(pieces_ref, 0, mm(c * sigmoid(c), d_mixed * wide_ref[...]))
    d_mixed_ref[...] = d_mixed
    grad_z_ref[...] = (d_gated * mixed * (sig * (1.0 + z * (1.0 - sig)))).astype(BF16)


def project_kernel(*refs):
    plane, row = refs[0][0], refs[0][1]
    part_refs, near_ref, far_ref = refs[1:5], refs[5], refs[6]
    own_ref, share_refs, left_ref = refs[7], refs[8:15], refs[15]
    tok = near_ref.shape[1]
    planes, rows = part_refs[0].shape[1], part_refs[0].shape[2]
    for step in range(planes):
        for k, part_ref in enumerate(part_refs):
            for half in (0, 1):
                at = (2 * k + half) * tok
                left_ref[step * rows : (step + 1) * rows, at : at + tok] = part_ref[
                    half, (plane + step) & (planes - 1)
                ]
    total = None
    for k in range(4):
        for half, block_ref in enumerate((near_ref, far_ref)):
            at = (2 * k + half) * tok
            term = mm(left_ref[:, at : at + tok], block_ref[(row - k) & 3])
            total = term if total is None else total + term
    own_ref[...] = total[:rows]
    for step in range(1, planes):
        share_refs[step - 1][...] = total[step * rows : (step + 1) * rows].astype(BF16)


def inside_back_kernel(
    x_ref, b_ref, c_ref, raw_ref, rate_ref, skip_ref, start_ref, wide_ref, d_mixed_ref,
    grad_x_ref, reach_x_ref, reach_s_ref, at_end_ref, d_b_ref, grad_c_ref, small_ref,
    d_scaled_ref,
):
    step, running = clocks(raw_ref[...], rate_ref[...])
    tok, heads = step.shape
    wide = x_ref.shape[1]
    last = running[-1:, :]
    spread = exact(
        jnp.concatenate(
            [step, jnp.exp(last - running), jnp.broadcast_to(skip_ref[...], (8, heads))], axis=0
        ),
        head_lanes(heads, wide),
    )
    step_wide, end_wide = spread[:tok], spread[tok : 2 * tok]
    x = x_ref[...].astype(F32)
    sig = sigmoid(x)
    x_act = x * sig
    scaled = x_act * step_wide
    d_mixed = d_mixed_ref[...]
    b, c = b_ref[...].astype(F32), c_ref[...].astype(F32)
    sig_c = sigmoid(c)
    b_t, c_t = b * sigmoid(b), c * sig_c
    b_act, c_act = b_t.T, c_t.T
    scores, scores_t = mm(c_act, b_t), mm(b_act, c_t)
    running_t = running.T
    rows, cols = iota((tok, tok), 0), iota((tok, tok), 1)
    keep, keep_t = rows >= cols, rows <= cols
    d_scores = jnp.zeros((tok, tok), F32)
    gained = jnp.zeros((tok, heads), F32)
    lost = jnp.zeros((heads, tok), F32)
    head_at, head_row = iota((tok, heads), 1), iota((heads, tok), 0)
    for pair in range(heads // 2):
        lanes = slice(pair * LANES, (pair + 1) * LANES)
        d_parts = halves(d_mixed[:, lanes])
        mixes_t = []
        for half in (0, 1):
            h = 2 * pair + half
            column, row = running[:, h : h + 1], running_t[h : h + 1, :]
            fade = fade_of(column, row, keep)
            mixes_t.append(scores_t * jnp.exp(jnp.where(keep_t, row - column, -1e30)))
            d_fade = mm_nt(d_parts[half], scaled[:, lanes]) * fade
            d_scores = d_scores + d_fade
            flow = d_fade * scores
            gained = jnp.where(head_at == h, jnp.sum(flow, axis=1, keepdims=True), gained)
            lost = jnp.where(head_row == h, jnp.sum(flow, axis=0, keepdims=True), lost)
        d_scaled_ref[:, lanes] = mm(
            jnp.concatenate(mixes_t, axis=1), jnp.concatenate(d_parts, axis=0)
        )
    start = start_ref[...].astype(F32)
    d_carried = d_mixed * wide_ref[...]
    by_head = head_rows(heads, wide)
    d_scaled = d_scaled_ref[...]
    d_run = gained - lost.T + exact(d_carried * mm(c_act, start), by_head)
    d_step = exact(d_scaled * x_act, by_head)
    small_ref[0] = d_run
    small_ref[1] = d_step
    small_ref[2] = jnp.broadcast_to(jnp.exp(last), (tok, heads))
    d_silu = sig * (1.0 + x * (1.0 - sig))
    grad_x_ref[...] = (d_scaled * step_wide + d_mixed * spread[2 * tok : 2 * tok + 1]) * d_silu
    reach_x_ref[...] = end_wide * step_wide * d_silu
    reach_s_ref[...] = end_wide * x_act
    at_end_ref[...] = (scaled * end_wide).astype(BF16)
    d_b_ref[...] = mm(c_t, d_scores)
    d_c = mm_nt(b_t, d_scores) + mm_nt(start, d_carried)
    grad_c_ref[...] = d_c * (sig_c * (1.0 + c * (1.0 - sig_c)))


def leave_kernel(
    pieces_ref, start_ref, b_ref, raw_ref, rate_ref, base_ref, reach_x_ref, reach_s_ref,
    at_end_ref, d_b_ref, small_ref, grad_x_ref, grad_b_ref, grad_step_ref,
):
    after = get_pieces(pieces_ref[...].astype(F32))
    b = b_ref[...].astype(F32)
    sig_b = sigmoid(b)
    reach = mm((b * sig_b).T, after)
    grad_x_ref[...] = (base_ref[...] + reach * reach_x_ref[...]).astype(BF16)
    tok, wide = reach.shape
    raw = raw_ref[...]
    step = softplus(raw).T
    heads = step.shape[1]
    both = jnp.concatenate(
        [
            reach * reach_s_ref[...],
            jnp.broadcast_to(
                jnp.sum(after * start_ref[...].astype(F32), axis=0, keepdims=True), (8, wide)
            ),
        ],
        axis=0,
    )
    sums = exact(both, head_rows(heads, wide))
    lost = step * sums[:tok]
    d_run = small_ref[0] - lost
    end_part = jnp.sum(lost, axis=0, keepdims=True) + small_ref[2][:1] * sums[tok : tok + 1]
    onward = (iota((tok, tok), 0) <= iota((tok, tok), 1)).astype(F32)
    d_log = exact(onward, d_run) + end_part
    d_step = small_ref[1] + sums[:tok] - d_log * rate_ref[...]
    grad_step_ref[...] = d_step.T * sigmoid(raw)
    d_b = d_b_ref[...] + mm_nt(after, at_end_ref[...])
    grad_b_ref[...] = d_b * (sig_b * (1.0 + b * (1.0 - sig_b)))


class Held:
    def __init__(self, array, late=False):
        self.array, self.late = array, late


def local(kernel, outs, args, flops, scratch=(), scalars=0, away=()):
    outs = outs if isinstance(outs, tuple) else (outs,)
    outs = tuple(pltpu.HBM(o.shape, o.dtype) if i in away else o for i, o in enumerate(outs))
    held = [i for i, a in enumerate(args) if isinstance(a, Held)]
    held.sort(key=lambda i: args[i].late)
    arrays = [
        pltpu.with_memory_space_constraint(a.array, pltpu.HBM) if isinstance(a, Held) else a
        for a in args
    ]
    spaces = [
        pltpu.SMEM if i < scalars else pltpu.HBM if i in held else pltpu.VMEM
        for i in range(len(args))
    ]
    count = len(args) + len(outs) + len(scratch)

    def run(*refs):
        refs, inside, sems = list(refs[:count]), refs[count:-1], refs[-1]
        copies = []
        for k, i in enumerate(held):
            copy = pltpu.make_async_copy(refs[i], inside[k], sems.at[k])
            copy.start()
            if args[i].late:
                refs[i] = (inside[k], copy)
            else:
                refs[i] = inside[k]
                copies.append(copy)
        for copy in copies:
            copy.wait()
        kernel(*refs)

    call = pl.pallas_call(
        run if held else kernel,
        out_shape=outs,
        scratch_shapes=(
            *scratch,
            *[pltpu.VMEM(arrays[i].shape, arrays[i].dtype) for i in held],
            *([pltpu.SemaphoreType.DMA((len(held),))] if held else []),
        ),
        in_specs=[pl.BlockSpec(memory_space=space) for space in spaces],
        compiler_params=pltpu.CompilerParams(vmem_limit_bytes=16 << 20),
        cost_estimate=pl.CostEstimate(flops=flops, bytes_accessed=1 << 21, transcendentals=1 << 18),
    )
    found = call(*arrays)
    return found if len(outs) > 1 else found[0]


def body(
    moe_input,
    cotangent,
    expert_ids,
    routing_weights,
    gate_weight,
    up_weight,
    down_weight,
    inner_x,
    inner_b,
    inner_c,
    gate_z,
    step_raw,
    decay_rate,
    skip_weight,
    norm_gain,
    w_out,
):
    tok = expert_ids.shape[0]
    heads = decay_rate.shape[0]
    experts = lax.axis_size(SP)
    wide = inner_x.shape[1]
    gate_w, up_w, down_w = gate_weight[0], up_weight[0], down_weight[0]
    ids_t, b_t, c_t, raw_t = expert_ids.T, inner_b.T, inner_c.T, step_raw.T
    rate, skip, gain = decay_rate[None, :], skip_weight[None, :], norm_gain[None, :]
    here = lax.axis_index("x")[None]
    shape = jax.ShapeDtypeStruct
    slots = experts * SLOTS
    cols, inner = moe_input.shape[1], gate_w.shape[1]

    sent_in = local(
        enter_kernel, shape((experts, 32, LANES), BF16), (Held(ids_t), Held(moe_input)), SMALL
    )
    got_in = to_all(sent_in, SP)
    sent_grad = local(
        weigh_kernel,
        shape((experts, 48, LANES), BF16),
        (Held(ids_t), Held(routing_weights.T), Held(cotangent), Held(inner_x), Held(b_t), Held(raw_t), Held(rate)),
        SMALL,
    )
    got_grad = to_all(sent_grad, SP)

    rows_in = rows_of(got_in)
    in_left, in_right, in_far = around(rows_in)
    pre, up_pre = local(
        first_kernel,
        (shape((slots, inner), F32), shape((slots, inner), F32)),
        (here, rows_in, in_left, in_right, in_far, Held(gate_w), Held(up_w)),
        SMALL,
        scalars=1,
        away=(0, 1),
    )
    rows_grad = rows_of(got_grad[:, :32])
    grad_left, grad_right, grad_far = around(rows_grad)

    pieces = local(ahead_kernel, shape((experts, 8, LANES), BF16), (got_grad,), SMALL)
    pieces = to_all(pieces, SP)

    down_near, gate_near, up_near, pre_near, up_pre_near = staged(
        (down_w, gate_w, up_w, pre, up_pre)
    )
    hidden, gate_grad, up_grad, term_far = local(
        hidden_kernel,
        (
            shape((slots, inner), BF16),
            shape((slots, inner), BF16),
            shape((slots, inner), BF16),
            shape((slots, cols), BF16),
        ),
        (
            here, rows_grad, grad_left, grad_right, grad_far, down_near, pre_near, up_pre_near,
            gate_near, up_near,
        ),
        SMALL,
        scalars=1,
        away=(0,),
    )
    term_far = shifted(term_far, 2)
    term_next, term_back, term_own = local(
        terms_kernel,
        (shape((slots, cols), BF16), shape((slots, cols), BF16), shape((slots, cols), BF16)),
        (here, gate_grad, up_grad, gate_near, up_near),
        SMALL,
        scalars=1,
        away=(2,),
    )
    terms = shifted(term_next, 1), shifted(term_back, -1)
    own_near = staged((term_own,))[0]
    slot_grad = local(sum_kernel, shape((slots, cols), BF16), (own_near, *terms, term_far), SMALL)

    norm_rows, mixed, start_state, start_wide = local(
        forward_kernel,
        (
            shape((tok, wide), BF16),
            shape((tok, wide), F32),
            shape((STATE, wide), BF16),
            shape((tok, wide), F32),
        ),
        (Held(inner_x), Held(gate_z), Held(b_t), Held(c_t), Held(raw_t), Held(rate), Held(skip), Held(gain), pieces),
        SMALL,
        away=(1, 2, 3),
    )
    norm_y = to_all(jnp.broadcast_to(norm_rows[None], (4, tok, wide)), "y")
    slot_grad, norm_y = lax.optimization_barrier((slot_grad, norm_y))
    back = to_all(slot_grad.reshape(experts, SLOTS, -1), SP).reshape(slots, -1)
    norm_c = along(norm_y, "c", 1)
    gate_out, up_out, down_out = local(
        weights_kernel,
        (
            shape(gate_w.shape, BF16),
            shape(up_w.shape, BF16),
            shape(down_w.shape, BF16),
        ),
        (
            here,
            *[
                Held(a)
                for a in (
                    rows_in, in_left, in_right, in_far, rows_grad, grad_left, grad_right, grad_far,
                    hidden, gate_grad, up_grad,
                )
            ],
        ),
        LARGE,
        scalars=1,
    )

    mixer_cols = local(
        combine_kernel,
        shape((4, *cotangent.shape), BF16),
        (Held(ids_t), Held(cotangent), back),
        SMALL,
    )
    mixer4 = to_all(mixer_cols, "x")
    mixed_near, wide_near = staged((mixed, start_wide))

    pieces, grad_z, d_mixed = local(
        gate_back_kernel,
        (
            shape((experts, 8, LANES), BF16),
            shape((tok, wide), BF16),
            shape((tok, wide), F32),
        ),
        (mixer4, Held(w_out, True), mixed_near, Held(gate_z), Held(gain), wide_near, Held(c_t)),
        SMALL,
        away=(2,),
    )

    mine, row, plane = lax.axis_index("c"), lax.axis_index("y"), lax.axis_index("z")
    mixer_t = mixer4.transpose(0, 2, 1).reshape(8, 4, 2, 32, tok).transpose(2, 1, 0, 3, 4)
    pieces = to_all(pieces, SP)
    keep = lax.dynamic_index_in_dim(mixer_t, mine, 0, keepdims=False)
    give = lax.dynamic_index_in_dim(mixer_t, 1 - mine, 0, keepdims=False)
    take = along(give, "c", 1)
    both = jnp.stack([keep, take], axis=0)
    parts = [lax.dynamic_index_in_dim(both, row, 1, keepdims=False)] + [
        along(lax.dynamic_index_in_dim(both, (row + step) % 4, 1, keepdims=False), "y", step)
        for step in (1, 2, 3)
    ]
    found = local(
        project_kernel,
        (shape((32, wide), F32), *[shape((32, wide), BF16)] * 7),
        (jnp.stack([plane, row]), *parts, norm_y, norm_c),
        SMALL,
        (pltpu.VMEM((256, 8 * tok), BF16),),
        scalars=1,
    )
    grad_out = found[0]
    for step in (4, 3, 5, 2, 6, 1, 7):
        share = along(found[step], "z", step)
        grad_out = grad_out + share.astype(F32)
    pieces = local(behind_kernel, shape((experts, 8, LANES), BF16), (got_grad, pieces), SMALL)
    pieces = to_all(pieces, SP)
    grad_x, reach_x, reach_s, at_end, d_b, grad_c, small = local(
        inside_back_kernel,
        (
            shape((tok, wide), F32),
            shape((tok, wide), F32),
            shape((tok, wide), F32),
            shape((tok, wide), BF16),
            shape((STATE, tok), F32),
            shape((STATE, tok), F32),
            shape((3, tok, heads), F32),
        ),
        (Held(inner_x), Held(b_t), Held(c_t), Held(raw_t), Held(rate), Held(skip), Held(start_state), Held(start_wide), Held(d_mixed)),
        LARGE,
        (pltpu.VMEM((tok, wide), F32),),
        away=tuple(range(7)),
    )
    grad_x, grad_b, grad_step = local(
        leave_kernel,
        (shape((tok, wide), BF16), shape((STATE, tok), F32), shape((heads, tok), F32)),
        (
            pieces,
            *[
                Held(a)
                for a in (start_state, b_t, raw_t, rate, grad_x, reach_x, reach_s, at_end, d_b, small)
            ],
        ),
        SMALL,
    )
    return (
        gate_out[None],
        up_out[None],
        down_out[None],
        grad_out,
        grad_x,
        grad_b.T,
        grad_c.T,
        grad_z,
        grad_step.T,
    )


def solution(mesh):
    finer = Mesh(mesh.devices.reshape(8, 4, 2, mesh.shape["tp"]), ("z", "y", "c", "x"))
    return jax.shard_map(
        body,
        mesh=finer,
        in_specs=(
            P(SP, "x"),
            P(SP, "x"),
            P(SP, None),
            P(SP, None),
            P(SP, None, "x"),
            P(SP, None, "x"),
            P(SP, "x", None),
            P(SP, "x"),
            P(SP, "x"),
            P(SP, "x"),
            P(SP, "x"),
            P(SP, "x"),
            P("x"),
            P("x"),
            P("x"),
            P(None, "x"),
        ),
        out_specs=(
            P(SP, None, "x"),
            P(SP, None, "x"),
            P(SP, "x", None),
            P(SP, "x"),
            P(SP, "x"),
            P(SP, "x"),
            P(SP, "x"),
            P(SP, "x"),
            P(SP, "x"),
        ),
        check_vma=False,
    )
```
